128 devices in a mesh: sp: 16 (over z, y), tp: 8 (over x, core).
Axes of the slice: x: 4, y: 4, z: 4, core: 2. Of those that a mesh axis runs over, the one named last changes fastest.
Arguments:
- hidden_activations: bfloat16 [12288, 4096], P(('sp', 'tp')), may hold values from -6 to 6
- entry_rescale_vector: bfloat16 [4096], replicated, may hold values from 0.099609375 to 1.8984375
- probe_matrix: bfloat16 [4096, 2048], P('sp', 'tp'), may hold values from -0.09375 to 0.09375
- lookup_address_matrix: bfloat16 [4096, 2048], P('sp', 'tp'), may hold values from -0.09375 to 0.09375
- payload_matrix: bfloat16 [4096, 4096], P('sp', 'tp'), may hold values from -0.09375 to 0.09375
- postfilter_switch_matrix: bfloat16 [4096, 4096], P('sp', 'tp'), may hold values from -0.09375 to 0.09375
- prefilter_switch_matrix: bfloat16 [4096, 4096], P('sp', 'tp'), may hold values from -0.09375 to 0.09375
- filter_source_matrix: bfloat16 [4096, 4096], P('sp', 'tp'), may hold values from -0.09375 to 0.09375
- forget_left_factor: bfloat16 [4096, 64], replicated, may hold values from -0.09375 to 0.09375
- forget_right_factor: bfloat16 [64, 2048], P(None, 'tp'), may hold values from -0.75 to 0.75
- forget_offset_per_feature: float32 [2048], P('tp'), may hold values from -1 to 12
- forget_spike_additions: float32 [16, 12288], P('tp', 'sp'), may hold values from -3 to 0
- subspace_rescale_vector: bfloat16 [16, 256], P('tp'), may hold values from 0.099609375 to 1.8984375
- depthwise_filter_taps: bfloat16 [3, 4096], P(None, 'tp'), may hold values from -3.5 to 3.5
- mixer_result_matrix: bfloat16 [4096, 4096], P('tp'), may hold values from -0.09375 to 0.09375
- filter_result_matrix: bfloat16 [4096, 4096], P('tp'), may hold values from -0.09375 to 0.09375
Outputs:
- mixed: bfloat16 [12288, 4096], P(('sp', 'tp'))
The draws below stay inside these ranges and needn't reach their ends.
All inputs are finite; a program needn't handle non-finite values.
Results may differ from the reference program's by a relative error of at most 0.02.
Values may be sent and summed in bfloat16 or wider, within the bound.
No kernel may reach another device: no remote copies, remote signals or barrier semaphores. Data moves between devices by JAX's collectives and lax.ppermute only.
A program may use at most 128 MiB of HBM per device.

```python
import jax
import jax.numpy as jnp
from jax import lax

MODEL = 4096
HEAD_TOTAL = 16
KEY_CHANNELS = 128
VALUE_DIM = 256
CONV_DIM = 4096
DECAY_RANK = 64
TAPS = 3
BLOCK = 64
TOKENS_DEV = 768
TOKEN_LENGTH = 12288
KEY_WIDTH = 2048
VALUE_WIDTH = 4096
N_TP = 8


def draw_forget_offset_per_feature(key, part):
    key_slow = jax.random.fold_in(key, 11)
    key_fast = jax.random.fold_in(key, 12)
    key_pick = jax.random.fold_in(key, 13)
    slow_heads = jax.random.randint(key_pick, (HEAD_TOTAL,), 0, 10) < 5
    slow_values = jnp.log(TOKEN_LENGTH / 8.0) + jax.random.uniform(key_slow, (HEAD_TOTAL, KEY_CHANNELS), jnp.float32, -0.5, 0.5)
    fast_values = jax.random.uniform(key_fast, (HEAD_TOTAL, KEY_CHANNELS), jnp.float32, -0.5, 1.5)
    chosen = jnp.where(slow_heads[:, None], slow_values, fast_values)
    return chosen.reshape(HEAD_TOTAL * KEY_CHANNELS).astype(jnp.float32)


def draw_forget_spike_additions(key, part):
    key_rate = jax.random.fold_in(key, 21)
    key_where = jax.random.fold_in(key, 22)
    key_size = jax.random.fold_in(key, 23)
    block_total = TOKEN_LENGTH // TOKENS_DEV
    rates = jnp.exp(jax.random.uniform(key_rate, (HEAD_TOTAL, block_total), jnp.float32, jnp.log(0.05), jnp.log(0.4)))
    starting_figure = -jnp.repeat(rates / TOKEN_LENGTH, TOKENS_DEV, axis=1)
    where = jax.random.randint(key_where, (HEAD_TOTAL, 3), 0, TOKEN_LENGTH)
    extent_sequence = jnp.log(jax.random.uniform(key_size, (HEAD_TOTAL, 3), jnp.float32, 0.5, 0.8))
    positions = jnp.arange(TOKEN_LENGTH, dtype=jnp.int32)
    agreeing_tally = (positions[None, None, :] == where[:, :, None]).astype(jnp.float32)
    spike_amounts = jnp.sum(agreeing_tally * extent_sequence[:, :, None], axis=1)
    return (starting_figure + spike_amounts).astype(jnp.float32)


def levels(stream_key, extent, pieces, low, largest):
    factor_of = 1.0
    for position, parts in pieces:
        steps = jax.random.uniform(jax.random.fold_in(jax.random.fold_in(stream_key, 6), position), (parts,), jnp.float32, low / len(pieces), largest / len(pieces))
        factor_of = factor_of * jnp.repeat(jnp.exp(steps), extent[position] // parts).reshape((-1,) + (1,) * (len(extent) - 1 - position))
    return factor_of


def scatter_about(key, shape, spread, bound, pieces=(), kind=jnp.bfloat16):
    level = levels(key, shape, pieces, -0.22, 0.18) if pieces else 1.0
    drawn = jax.random.normal(key, shape, jnp.float32) * spread * level
    return jnp.minimum(jnp.maximum(drawn, -bound), bound).astype(kind)


def setup_inputs(seed: int = 0) -> dict:
    key_of = jax.random.split(jax.random.key(seed), 17)
    return {
        "hidden_activations": scatter_about(key_of[0], (TOKEN_LENGTH, MODEL), 1.0, 6.0, ((0, 128),)),
        "entry_rescale_vector": jnp.clip(1.0 + 0.18 * jax.random.normal(key_of[1], (MODEL,), jnp.float32), 0.099609375, 1.8984375).astype(jnp.bfloat16),
        "probe_matrix": scatter_about(key_of[2], (MODEL, KEY_WIDTH), MODEL ** -0.5, 0.09375, ((0, 16), (1, 8))),
        "lookup_address_matrix": scatter_about(key_of[3], (MODEL, KEY_WIDTH), MODEL ** -0.5, 0.09375, ((0, 16), (1, 8))),
        "payload_matrix": scatter_about(key_of[4], (MODEL, VALUE_WIDTH), MODEL ** -0.5, 0.09375, ((0, 16), (1, 8))),
        "postfilter_switch_matrix": scatter_about(key_of[5], (MODEL, CONV_DIM), MODEL ** -0.5, 0.09375, ((0, 16), (1, 8))),
        "prefilter_switch_matrix": scatter_about(key_of[6], (MODEL, CONV_DIM), MODEL ** -0.5, 0.09375, ((0, 16), (1, 8))),
        "filter_source_matrix": scatter_about(key_of[7], (MODEL, CONV_DIM), MODEL ** -0.5, 0.09375, ((0, 16), (1, 8))),
        "forget_left_factor": scatter_about(key_of[8], (MODEL, DECAY_RANK), MODEL ** -0.5, 0.09375),
        "forget_right_factor": scatter_about(key_of[9], (DECAY_RANK, KEY_WIDTH), DECAY_RANK ** -0.5, 0.75, ((1, 8),)),
        "forget_offset_per_feature": draw_forget_offset_per_feature(jax.random.fold_in(key_of[16], 71), 0),
        "forget_spike_additions": draw_forget_spike_additions(jax.random.fold_in(key_of[16], 71), 0),
        "subspace_rescale_vector": jnp.clip(1.0 + 0.18 * jax.random.normal(key_of[12], (HEAD_TOTAL, VALUE_DIM), jnp.float32), 0.099609375, 1.8984375).astype(jnp.bfloat16),
        "depthwise_filter_taps": scatter_about(key_of[13], (TAPS, CONV_DIM), TAPS ** -0.5, 3.5, ((1, 8),)),
        "mixer_result_matrix": scatter_about(key_of[14], (VALUE_WIDTH, MODEL), VALUE_WIDTH ** -0.5, 0.09375, ((0, 8),)),
        "filter_result_matrix": scatter_about(key_of[15], (CONV_DIM, MODEL), CONV_DIM ** -0.5, 0.09375, ((0, 8),)),
    }


epsilon = 1e-06
softness_scale = 16.0

def row_norm(rows, gain):
    rows_f = rows.astype(jnp.float32)
    meansq = lax.optimization_barrier(jnp.mean(rows_f * rows_f, axis=-1, keepdims=True))
    return rows_f * lax.rsqrt(meansq + epsilon) * gain.astype(jnp.float32)

def block_terms(query_rows, key_rows, value_rows, forget_log_rate):
    length_value, head_number, key_dim = query_rows.shape
    value_dim = value_rows.shape[2]
    block_count = length_value // BLOCK
    key_shape = (block_count, BLOCK, head_number, key_dim)
    query_f32 = query_rows.astype(jnp.float32).reshape(key_shape) * key_dim ** (-0.5)
    key_f32 = key_rows.astype(jnp.float32).reshape(key_shape)
    value_f32 = value_rows.astype(jnp.float32).reshape(block_count, BLOCK, head_number, value_dim)
    within = jnp.cumsum(forget_log_rate.reshape(key_shape), axis=1)
    block_end = within[:, -1]
    query_decayed = query_f32 * jnp.exp(within)
    key_inverse = key_f32 * jnp.exp(-within)
    key_tail = key_f32 * jnp.exp(block_end[:, None] - within)
    highest = lax.Precision.HIGHEST
    scores = jnp.einsum('nihd,njhd->nhij', query_decayed, key_inverse, precision=highest)
    causal = jnp.tril(jnp.ones((BLOCK, BLOCK), dtype=bool))
    scores = jnp.where(causal, scores, 0.0)
    inside = jnp.einsum('nhij,njhv->nihv', scores, value_f32, precision=highest)
    updates = jnp.einsum('njhd,njhv->nhdv', key_tail, value_f32, precision=highest)

    def advance(state, pair):
        decay_now, update_now = pair
        return (jnp.exp(decay_now)[..., None] * state + update_now, state)
    start_state = jnp.zeros((head_number, key_dim, value_dim), jnp.float32)
    final_state, state_in = lax.scan(advance, start_state, (block_end, updates))
    carried = jnp.einsum('nihd,nhdv->nihv', query_decayed, state_in, precision=highest)
    return (inside + carried, query_decayed, block_end, final_state)

def reference(hidden_activations, entry_rescale_vector, probe_matrix, lookup_address_matrix, payload_matrix, postfilter_switch_matrix, prefilter_switch_matrix, filter_source_matrix, forget_left_factor, forget_right_factor, forget_offset_per_feature, forget_spike_additions, subspace_rescale_vector, depthwise_filter_taps, mixer_result_matrix, filter_result_matrix):
    normalized_input = row_norm(hidden_activations, entry_rescale_vector).astype(jnp.bfloat16)

    def project(weight):
        return jnp.dot(normalized_input, weight, preferred_element_type=jnp.float32).astype(jnp.bfloat16)
    queries = project(probe_matrix)
    key_rows = project(lookup_address_matrix)
    value_rows = project(payload_matrix)
    outer = project(postfilter_switch_matrix)
    inner = project(prefilter_switch_matrix)
    conv_in = project(filter_source_matrix)
    low_rank = project(forget_left_factor)
    gate_preactivation = jnp.dot(low_rank, forget_right_factor, preferred_element_type=jnp.float32) + forget_offset_per_feature
    forget_log_rate = (jax.nn.log_sigmoid(gate_preactivation) / softness_scale).reshape(TOKEN_LENGTH, HEAD_TOTAL, KEY_CHANNELS)
    forget_log_rate = forget_log_rate + jnp.transpose(forget_spike_additions)[:, :, None]
    attended, unused_q, unused_e, unused_s = block_terms(queries.reshape(TOKEN_LENGTH, HEAD_TOTAL, KEY_CHANNELS), key_rows.reshape(TOKEN_LENGTH, HEAD_TOTAL, KEY_CHANNELS), value_rows.reshape(TOKEN_LENGTH, HEAD_TOTAL, VALUE_DIM), forget_log_rate)
    attended = attended.reshape(TOKEN_LENGTH, HEAD_TOTAL, VALUE_DIM)
    mixed_attn = row_norm(attended, subspace_rescale_vector).astype(jnp.bfloat16).reshape(TOKEN_LENGTH, HEAD_TOTAL * VALUE_DIM)
    gated_in = (inner.astype(jnp.float32) * conv_in.astype(jnp.float32)).astype(jnp.bfloat16)
    padded = jnp.concatenate([jnp.zeros((TAPS - 1, CONV_DIM), jnp.bfloat16), gated_in], axis=0)
    taps_f32 = depthwise_filter_taps.astype(jnp.float32)
    conv_sum = jnp.zeros((TOKEN_LENGTH, CONV_DIM), jnp.float32)
    for tap_index in range(TAPS):
        conv_sum = conv_sum + taps_f32[tap_index] * padded[tap_index:tap_index + TOKEN_LENGTH].astype(jnp.float32)
    mixed_conv = (conv_sum * outer.astype(jnp.float32)).astype(jnp.bfloat16)
    head_cols = HEAD_TOTAL * VALUE_DIM // N_TP
    conv_cols = CONV_DIM // N_TP
    running = jnp.zeros((TOKEN_LENGTH, MODEL), jnp.float32)
    for group in range(N_TP):
        term = jnp.dot(mixed_attn[:, group * head_cols:(group + 1) * head_cols], mixer_result_matrix[group * head_cols:(group + 1) * head_cols], preferred_element_type=jnp.float32)
        term = term + jnp.dot(mixed_conv[:, group * conv_cols:(group + 1) * conv_cols], filter_result_matrix[group * conv_cols:(group + 1) * conv_cols], preferred_element_type=jnp.float32)
        rounded = lax.optimization_barrier(term.astype(jnp.bfloat16))
        running = running + rounded.astype(jnp.float32)
    return running.astype(jnp.bfloat16)
```

```python
import jax
import jax.numpy as jnp
from jax import lax
from jax.experimental import pallas as pl
from jax.experimental.pallas import tpu as pltpu
from jax.sharding import Mesh
from jax.sharding import PartitionSpec as P

BLOCK = 64
SP = ("z", "y")
TP = ("x", "c")
ALL = ("z", "y", "x", "c")
RING = 4
PAIR = 2
HALO = 16

EPSILON = 1e-06
SOFTNESS = 16.0

F32 = jnp.float32
BF16 = jnp.bfloat16


def dot(a, b):
    return jnp.dot(a, b, preferred_element_type=F32)


def hop(value, axis, steps):
    return lax.ppermute(value, axis, [(i, (i + steps) % RING) for i in range(RING)])


def swap(value):
    return lax.ppermute(value, "c", [(0, 1), (1, 0)])


def onward(value, axis, steps):
    count = RING * RING if axis == SP else RING
    return lax.ppermute(value, axis, [(i, i + steps) for i in range(count - steps)])


def around(value, axis):
    half = value.shape[0] // 2
    below, above = hop(value, axis, 1), hop(value, axis, -1)
    return (
        (value, 0, 0),
        (below, 3, 0),
        (above, 1, 0),
        (hop(below[:half], axis, 1), 2, 0),
        (hop(above[half:], axis, -1), 2, half),
    )


def place(buffer, block, starts):
    block = block.reshape((1,) * (buffer.ndim - block.ndim) + block.shape)
    return lax.dynamic_update_slice(buffer, block, starts)


def gather_tp(shard):
    x, c = lax.axis_index("x"), lax.axis_index("c")
    out = jnp.zeros((RING, PAIR) + shard.shape, shard.dtype)
    for block, step, offset in around(shard, "x"):
        at = (x + step) % RING
        out = place(out, block, (at, c, offset, 0))
        out = place(out, swap(block), (at, 1 - c, offset, 0))
    return out.reshape(RING * PAIR * shard.shape[0], shard.shape[1])


def gather_sp(shard):
    half = shard.shape[0] // 2
    width = shard.shape[1]
    out = jnp.zeros((RING, RING, 2, half, width), shard.dtype)
    z, y = lax.axis_index("z"), lax.axis_index("y")
    for order, piece in enumerate((shard[:half], shard[half:])):
        first, second = ("y", "z") if order == 0 else ("z", "y")
        here, there = (y, z) if order == 0 else (z, y)
        line = jnp.zeros((RING, half, width), shard.dtype)
        for block, step, offset in around(piece, first):
            line = place(line, block, ((here + step) % RING, offset, 0))
        for lines, step, offset in around(line, second):
            at = (there + step) % RING
            if order == 0:
                out = lax.dynamic_update_slice(
                    out, lines[None, :, None], (at, offset, order, 0, 0)
                )
            else:
                out = lax.dynamic_update_slice(
                    out, lines[:, None, None], (offset, at, order, 0, 0)
                )
    return out.reshape(RING * RING * 2 * half, width)


def norm_values(rows, gain):
    rows_f = rows.astype(F32)
    meansq = jnp.mean(rows_f * rows_f, axis=-1, keepdims=True)
    return rows_f * lax.rsqrt(meansq + EPSILON) * gain.astype(F32)


def decay_kernel(rate_ref, in_ref, out_ref, tail_ref, far_ref, end_ref, total_ref):
    blocks = rate_ref.shape[0] // BLOCK
    low = lax.broadcasted_iota(jnp.int32, (BLOCK, BLOCK), 0)
    high = lax.broadcasted_iota(jnp.int32, (BLOCK, BLOCK), 1)
    tri = jnp.where(high <= low, 1.0, 0.0).astype(F32)
    prefix = jnp.zeros((1, rate_ref.shape[1]), F32)
    for n in range(blocks):
        rows = slice(n * BLOCK, (n + 1) * BLOCK)
        within = jnp.dot(
            tri, rate_ref[rows], preferred_element_type=F32, precision=lax.Precision.HIGHEST
        )
        end = within[BLOCK - 1 :]
        grow = jnp.exp(within)
        in_ref[rows] = grow
        out_ref[rows] = jnp.exp(-within)
        tail_ref[rows] = jnp.exp(end - within)
        far_ref[rows] = grow * jnp.exp(prefix)
        end_ref[n : n + 1] = jnp.exp(end)
        prefix = prefix + end
    total_ref[...] = jnp.exp(prefix)


def decay_terms(rate):
    length, width = rate.shape
    full = jax.ShapeDtypeStruct((length, width), F32)
    return pl.pallas_call(
        decay_kernel,
        out_shape=(
            full,
            full,
            full,
            full,
            jax.ShapeDtypeStruct((length // BLOCK, width), F32),
            jax.ShapeDtypeStruct((1, width), F32),
        ),
        cost_estimate=pl.CostEstimate(
            flops=4_000_000_000, bytes_accessed=4_000_000, transcendentals=1_000_000
        ),
    )(rate)


def across(a, b):
    return lax.dot_general(a, b, (((1,), (1,)), ((), ())), preferred_element_type=F32)


def local_kernel(q_ref, k_ref, v_ref, in_ref, out_ref, tail_ref, far_ref, end_ref, part_ref, qfar_ref, state_ref):
    length = q_ref.shape[0]
    heads = state_ref.shape[0]
    key_dim = q_ref.shape[1] // heads
    value_dim = v_ref.shape[1] // heads
    scale = key_dim ** (-0.5)
    low = lax.broadcasted_iota(jnp.int32, (BLOCK, BLOCK), 0)
    high = lax.broadcasted_iota(jnp.int32, (BLOCK, BLOCK), 1)
    causal = high <= low
    states = [jnp.zeros((value_dim, key_dim), F32) for _ in range(heads)]
    for n in range(length // BLOCK):
        rows = slice(n * BLOCK, (n + 1) * BLOCK)
        for h in range(heads):
            keys = slice(h * key_dim, (h + 1) * key_dim)
            values = slice(h * value_dim, (h + 1) * value_dim)
            q = q_ref[rows, keys].astype(F32) * scale
            k = k_ref[rows, keys].astype(F32)
            v = v_ref[rows, values]
            qd = (q * in_ref[rows, keys]).astype(BF16)
            ki = (k * out_ref[rows, keys]).astype(BF16)
            kt = (k * tail_ref[rows, keys]).astype(BF16)
            qfar_ref[rows, keys] = (q * far_ref[rows, keys]).astype(BF16)
            scores = jnp.where(causal, across(qd, ki), 0.0).astype(BF16)
            part = dot(scores, v)
            if n > 0:
                part = part + across(qd, states[h].astype(BF16))
            part_ref[rows, values] = part
            update = lax.dot_general(v, kt, (((0,), (0,)), ((), ())), preferred_element_type=F32)
            states[h] = states[h] * end_ref[n : n + 1, keys] + update
    for h in range(heads):
        state_ref[h] = states[h]


def local_attention(q, k, v, terms, heads):
    length, width = q.shape
    wide = v.shape[1]
    return pl.pallas_call(
        local_kernel,
        out_shape=(
            jax.ShapeDtypeStruct((length, wide), F32),
            jax.ShapeDtypeStruct((length, width), BF16),
            jax.ShapeDtypeStruct((heads, wide // heads, width // heads), F32),
        ),
        cost_estimate=pl.CostEstimate(
            flops=12_000_000_000, bytes_accessed=8_000_000, transcendentals=0
        ),
    )(q, k, v, *terms)


def finish_kernel(part_ref, qfar_ref, state_ref, gain_ref, mixed_ref):
    heads = state_ref.shape[0]
    key_dim = qfar_ref.shape[1] // heads
    value_dim = part_ref.shape[1] // heads
    for h in range(heads):
        keys = slice(h * key_dim, (h + 1) * key_dim)
        values = slice(h * value_dim, (h + 1) * value_dim)
        attended = part_ref[:, values] + across(qfar_ref[:, keys], state_ref[h])
        meansq = jnp.mean(attended * attended, axis=-1, keepdims=True)
        gain = gain_ref[h : h + 1].astype(F32)
        mixed_ref[:, values] = (attended * lax.rsqrt(meansq + EPSILON) * gain).astype(BF16)


def finish_attention(part, qfar, state, gain):
    length, wide = part.shape
    tile = 96
    return pl.pallas_call(
        finish_kernel,
        grid=(length // tile,),
        in_specs=[
            pl.BlockSpec((tile, wide), lambda i: (i, 0)),
            pl.BlockSpec((tile, qfar.shape[1]), lambda i: (i, 0)),
            pl.BlockSpec(state.shape, lambda i: (0, 0, 0)),
            pl.BlockSpec(gain.shape, lambda i: (0, 0)),
        ],
        out_specs=pl.BlockSpec((tile, wide), lambda i: (i, 0)),
        out_shape=jax.ShapeDtypeStruct((length, wide), BF16),
        cost_estimate=pl.CostEstimate(
            flops=3_000_000_000, bytes_accessed=3_000_000, transcendentals=1000
        ),
    )(part, qfar, state, gain)


def unpack(packed, value_dim):
    packed = packed.astype(F32)
    return packed[:, value_dim : value_dim + 1], packed[:, :value_dim]


def combine(earlier, later):
    return earlier[0] * later[0], later[0] * earlier[1] + later[1]


def pack(pair):
    decay, state = pair
    heads, _, key_dim = state.shape
    lines = jnp.broadcast_to(decay, (heads, 16, key_dim))
    return jnp.concatenate([state, lines], axis=1).astype(BF16)


def entering(decay, state):
    value_dim = state.shape[1]
    z, y = lax.axis_index("z"), lax.axis_index("y")
    own = pack((decay, state))
    empty = (jnp.ones_like(decay), jnp.zeros_like(state))

    def only(passed, pair):
        return tuple(jnp.where(passed, a, b) for a, b in zip(pair, empty))

    before = empty
    total = (decay, state)
    got = [unpack(hop(own, "y", step), value_dim) for step in (1, 2, 3)]
    for step in (1, 2, 3):
        pair = got[step - 1]
        before = combine(only(y >= step, pair), before)
    after = empty
    for step in (3, 2, 1):
        after = combine(after, only(y < step, got[step - 1]))
    total = combine(combine(before, total), after)
    line = pack(total)
    outer = empty
    for step in (1, 2, 3):
        pair = unpack(onward(line, "z", step), value_dim)
        outer = combine(only(z >= step, pair), outer)
    return combine(outer, before)[1].astype(BF16)


def conv_gate(sums, taps):
    width = sums.shape[1] // 3
    length = sums.shape[0] - HALO
    outer = sums[HALO:, :width].astype(F32)
    gated = (sums[:, width : 2 * width].astype(F32) * sums[:, 2 * width :].astype(F32)).astype(BF16)
    start = HALO + 1 - taps.shape[0]
    conv = jnp.zeros((length, width), F32)
    for i in range(taps.shape[0]):
        conv = conv + taps[i].astype(F32) * gated[start + i : start + i + length].astype(F32)
    return (conv * outer).astype(BF16)


def plus(*terms):
    total = terms[0].astype(F32)
    for term in terms[1:]:
        total = total + term.astype(F32)
    return total


def body(
    hidden,
    entry_gain,
    probe,
    lookup,
    payload,
    postfilter,
    prefilter,
    source,
    forget_left,
    forget_right,
    forget_offset,
    forget_spike,
    head_gain,
    taps,
    mixer_result,
    filter_result,
):
    heads, value_dim = head_gain.shape
    key_dim = probe.shape[1] // heads
    x, c = lax.axis_index("x"), lax.axis_index("c")

    w_conv = lax.all_gather(
        jnp.concatenate([postfilter, prefilter, source], axis=1), SP, axis=0, tiled=True
    )
    normed = gather_tp(norm_values(hidden, entry_gain).astype(BF16))
    w_attn = gather_sp(jnp.concatenate([probe, lookup, payload], axis=1))
    length = normed.shape[0]
    rim = onward(normed[length - HALO :], SP, 1)
    extended = jnp.concatenate([rim, normed], axis=0)

    low_rank = dot(normed, forget_left).astype(BF16)
    gate = dot(low_rank, forget_right) + forget_offset
    rate = (jax.nn.log_sigmoid(gate) / SOFTNESS).reshape(length, heads, key_dim)
    rate = (rate + jnp.transpose(forget_spike)[:, :, None]).reshape(length, heads * key_dim)
    *terms, total = decay_terms(rate)
    total = total.reshape(heads, 1, key_dim)

    sums = dot(normed, w_attn).astype(BF16)
    keys = heads * key_dim
    q, k, v = sums[:, :keys], sums[:, keys : 2 * keys], sums[:, 2 * keys :]
    near, qfar, state = local_attention(q, k, v, terms, heads)
    incoming = entering(total, state)
    mixed_attn = finish_attention(near, qfar, incoming, head_gain)

    w_out = jnp.concatenate([mixer_result, filter_result], axis=0)
    group = length // RING
    part = group // PAIR

    def partial(step):
        start = ((x + step) % RING) * group
        rows = lax.dynamic_slice_in_dim(extended, start, group + HALO, axis=0)
        conv = conv_gate(dot(rows, w_conv).astype(BF16), taps)
        attn = lax.dynamic_slice_in_dim(mixed_attn, start, group, axis=0)
        mixed = jnp.concatenate([attn, conv], axis=1).reshape(PAIR, part, -1)
        mixed = jnp.where(c == 0, mixed[::-1], mixed).reshape(group, -1)
        out = dot(mixed, w_out)
        return out[part:] + swap(out[:part].astype(BF16)).astype(F32)

    half = part // 2
    far = partial(2).astype(BF16)
    far_up, far_down = hop(far[:half], "x", 1), hop(far[half:], "x", -1)
    up = partial(1)
    up = jnp.concatenate([plus(up[:half], far_up), up[half:]], axis=0).astype(BF16)
    from_below = hop(up, "x", 1)
    down = partial(3)
    down = jnp.concatenate([down[:half], plus(down[half:], far_down)], axis=0).astype(BF16)
    from_above = hop(down, "x", -1)
    return plus(partial(0), from_below, from_above).astype(BF16)


def solution(mesh):
    split = Mesh(mesh.devices.reshape(RING, RING, RING, PAIR), ALL)
    in_specs = (
        P(ALL, None),
        P(),
        P(SP, TP),
        P(SP, TP),
        P(SP, TP),
        P(SP, TP),
        P(SP, TP),
        P(SP, TP),
        P(),
        P(None, TP),
        P(TP),
        P(TP, SP),
        P(TP, None),
        P(None, TP),
        P(TP, None),
        P(TP, None),
    )
    return jax.shard_map(
        body, mesh=split, in_specs=in_specs, out_specs=P(ALL, None), check_vma=False
    )
```

```python
import functools

import jax
import jax.numpy as jnp
from jax import lax
from jax.experimental import pallas as pl
from jax.experimental.pallas import tpu as pltpu
from jax.sharding import Mesh
from jax.sharding import PartitionSpec as P

BLOCK = 64
SP = ("z", "y")
TP = ("x", "c")
ALL = ("z", "y", "x", "c")
RING = 4
PAIR = 2
HALO = 16

EPSILON = 1e-06
SOFTNESS = 16.0

F32 = jnp.float32
BF16 = jnp.bfloat16


def dot(a, b):
    return jnp.dot(a, b, preferred_element_type=F32)


def hop(value, axis, steps):
    return lax.ppermute(value, axis, [(i, (i + steps) % RING) for i in range(RING)])


def swap(value):
    return lax.ppermute(value, "c", [(0, 1), (1, 0)])


def onward(value, axis, steps):
    count = RING * RING if axis == SP else RING
    return lax.ppermute(value, axis, [(i, i + steps) for i in range(count - steps)])


def around(value, axis, half=None):
    half = half or value.shape[0] // 2
    below, above = hop(value, axis, 1), hop(value, axis, -1)
    top = hop(below[:half], axis, 1)
    bottom = hop(above[half:], axis, -1)
    return value, below, above, top, bottom


def vmem_kernel(kernel, out_shape, flops, *args, **kwargs):
    return pl.pallas_call(
        kernel,
        out_shape=out_shape,
        compiler_params=pltpu.CompilerParams(vmem_limit_bytes=kwargs.pop("limit", 16) << 20),
        cost_estimate=pl.CostEstimate(
            flops=flops, bytes_accessed=8_000_000, transcendentals=0
        ),
        **kwargs,
    )(*args)


def line_kernel(axis, own, below, above, top, bottom, *outs):
    me = lax.axis_index(axis)
    rows = own.shape[0]
    half = rows // 2
    at = 0
    for out in outs:
        cols = slice(at, at + out.shape[1])
        at += out.shape[1]
        for ref, step, offset in (
            (own, 0, 0),
            (below, 3, 0),
            (above, 1, 0),
            (top, 2, 0),
            (bottom, 2, half),
        ):
            start = pl.multiple_of(lax.rem(me + step, RING) * rows + offset, half)
            out[pl.ds(start, ref.shape[0]), :] = ref[:, cols]


def line_up(axis, pieces, widths):
    rows = pieces[0].shape[0] * RING
    return vmem_kernel(
        functools.partial(line_kernel, axis),
        tuple(jax.ShapeDtypeStruct((rows, w), BF16) for w in widths),
        1_000_000_000,
        *pieces,
    )


def chips_kernel(own, below, above, top, bottom, out):
    x = lax.axis_index("x")
    rows = own.shape[0]
    half = top.shape[0]
    for ref, step, offset in (
        (own, 0, 0),
        (below, 3, 0),
        (above, 1, 0),
        (top, 2, 0),
        (bottom, 2, half),
    ):
        start = pl.multiple_of(lax.rem(x + step, RING) * rows + offset, HALO)
        out[pl.ds(start, ref.shape[0]), :] = ref[...]


def rows_kernel(mine, other, out):
    c = lax.axis_index("c")
    block = mine.shape[0] // RING
    part = block - HALO
    for ref, core in ((mine, c), (other, 1 - c)):
        for chip in range(RING):
            start = pl.multiple_of(HALO + (chip * PAIR + core) * part, HALO)
            out[pl.ds(start, part), :] = ref[chip * block : chip * block + part]

        @pl.when(core == 1)
        def _(ref=ref):
            out[:HALO] = ref[RING * block - HALO :]


def gather_rows(shard):
    block, width = shard.shape
    part = block - HALO
    pieces = around(shard, "x", part // 2)
    mine = vmem_kernel(
        chips_kernel, jax.ShapeDtypeStruct((RING * block, width), BF16), 1_000_000_000, *pieces
    )
    return vmem_kernel(
        rows_kernel,
        jax.ShapeDtypeStruct((HALO + RING * PAIR * part, width), BF16),
        2_000_000_000,
        mine,
        swap(mine),
    )


def project(x_ref, lead, along, pieces, which, block):
    me = lax.axis_index("z" if along == 0 else "y")
    total = None
    for ref, index in zip(pieces, which):
        step, first = ((0, 0), (3, 0), (1, 0), (2, 0), (2, 2))[index]
        where = lax.rem(me + step, RING)
        count = ref.shape[0] // block
        if along == 0:
            start = pl.multiple_of((where * RING + first) * block, block)
            term = dot(x_ref[lead:, pl.ds(start, count * block)], ref[...])
            total = term if total is None else total + term
        else:
            for i in range(count):
                start = pl.multiple_of(((first + i) * RING + where) * block, block)
                term = dot(
                    x_ref[lead:, pl.ds(start, block)], ref[i * block : (i + 1) * block, :]
                )
                total = term if total is None else total + term
    return total


def project_kernel(lead, along, which, block, x_ref, *refs):
    *pieces, out = refs
    out[...] = project(x_ref, lead, along, pieces, which, block).astype(out.dtype)


def project_more_kernel(lead, along, which, block, x_ref, acc_ref, *refs):
    *pieces, out = refs
    total = acc_ref[...] + project(x_ref, lead, along, pieces, which, block)
    out[...] = total.astype(out.dtype)


def project_call(x, acc, pieces, which, along, lead, dtype, tile=256):
    block = x.shape[1] // (RING * RING)
    rows = x.shape[0] - lead
    width = pieces[0].shape[1]
    more = () if acc is None else (acc,)
    kernel = project_kernel if acc is None else project_more_kernel
    return vmem_kernel(
        functools.partial(kernel, lead, along, which, block),
        jax.ShapeDtypeStruct((rows, width), dtype),
        3_000_000_000,
        x,
        *more,
        *pieces,
        grid=(width // tile,),
        in_specs=[pl.BlockSpec(memory_space=pltpu.VMEM)]
        + [pl.BlockSpec((rows, tile), lambda i: (0, i)) for _ in more]
        + [pl.BlockSpec((p.shape[0], tile), lambda i: (0, i)) for p in pieces],
        out_specs=pl.BlockSpec((rows, tile), lambda i: (0, i)),
    )


def gate_kernel(along, which, block, x_ref, acc_ref, *refs):
    *pieces, taps_ref, out = refs
    sums = (acc_ref[...] + project(x_ref, 0, along, pieces, which, block)).astype(BF16)
    width = sums.shape[1] // 3
    length = sums.shape[0] - HALO
    gated = (sums[:, width : 2 * width].astype(F32) * sums[:, 2 * width :].astype(F32)).astype(BF16)
    gated = gated.astype(F32)
    taps = taps_ref.shape[0]
    conv = jnp.zeros((length, width), F32)
    for i in range(taps):
        lead = HALO + 1 - taps + i
        conv = conv + taps_ref[i : i + 1, :].astype(F32) * gated[lead : lead + length]
    out[...] = (conv * sums[HALO:, :width].astype(F32)).astype(BF16)


def gate_call(x, acc, pieces, which, taps, along):
    block = x.shape[1] // (RING * RING)
    return vmem_kernel(
        functools.partial(gate_kernel, along, which, block),
        jax.ShapeDtypeStruct((x.shape[0] - HALO, taps.shape[1]), BF16),
        2_000_000_000,
        x,
        acc,
        *pieces,
        taps,
        in_specs=[pl.BlockSpec(memory_space=pltpu.VMEM)] * (3 + len(pieces)),
        out_specs=pl.BlockSpec(memory_space=pltpu.VMEM),
    )


def norm_values(rows, gain):
    rows_f = rows.astype(F32)
    meansq = jnp.mean(rows_f * rows_f, axis=-1, keepdims=True)
    return rows_f * lax.rsqrt(meansq + EPSILON) * gain.astype(F32)


def decay_kernel(
    x_ref, left_ref, right_ref, offset_ref, spike_ref, in_ref, out_ref, tail_ref, far_ref, end_ref, total_ref
):
    length, width = in_ref.shape
    heads = spike_ref.shape[0]
    low_rank = across(x_ref[HALO:, :], left_ref[...]).astype(BF16)
    gate = dot(low_rank, right_ref[...]) + offset_ref[...]
    soft = jnp.minimum(gate, 0.0) - jnp.log1p(jnp.exp(-jnp.abs(gate)))
    head = lax.broadcasted_iota(jnp.int32, (heads, width), 0)
    feature = lax.broadcasted_iota(jnp.int32, (heads, width), 1)
    owner = jnp.where(feature // (width // heads) == head, 1.0, 0.0).astype(F32)
    spikes = lax.dot_general(
        spike_ref[...],
        owner,
        (((0,), (0,)), ((), ())),
        preferred_element_type=F32,
        precision=lax.Precision.HIGHEST,
    )
    rate = soft / SOFTNESS + spikes
    low = lax.broadcasted_iota(jnp.int32, (BLOCK, BLOCK), 0)
    high = lax.broadcasted_iota(jnp.int32, (BLOCK, BLOCK), 1)
    tri = jnp.where(high <= low, 1.0, 0.0).astype(F32)
    prefix = jnp.zeros((1, width), F32)
    tail_ref[...] = rate

    def step(n, prefix):
        rows = pl.ds(pl.multiple_of(n * BLOCK, BLOCK), BLOCK)
        within = jnp.dot(
            tri, tail_ref[rows, :], preferred_element_type=F32, precision=lax.Precision.HIGHEST
        )
        end = within[BLOCK - 1 :]
        grow = jnp.exp(within)
        in_ref[rows, :] = grow
        out_ref[rows, :] = jnp.exp(-within)
        tail_ref[rows, :] = jnp.exp(end - within)
        far_ref[rows, :] = grow * jnp.exp(prefix)
        end_ref[pl.ds(n, 1), :] = jnp.exp(end)
        return prefix + end

    total_ref[...] = jnp.exp(lax.fori_loop(0, length // BLOCK, step, prefix))


def decay_terms(x, left, right, offset, spike):
    length, width = x.shape[0] - HALO, right.shape[1]
    full = jax.ShapeDtypeStruct((length, width), F32)
    return vmem_kernel(
        decay_kernel,
        (
            full,
            full,
            full,
            full,
            jax.ShapeDtypeStruct((length // BLOCK, width), F32),
            jax.ShapeDtypeStruct((1, width), F32),
        ),
        4_000_000_000,
        x,
        jnp.transpose(left),
        right,
        offset[None],
        spike,
        in_specs=[pl.BlockSpec(memory_space=pltpu.VMEM)] * 5,
    )


def across(a, b):
    return lax.dot_general(a, b, (((1,), (1,)), ((), ())), preferred_element_type=F32)


def local_kernel(qk_ref, v_ref, in_ref, out_ref, tail_ref, far_ref, end_ref, part_ref, qfar_ref, state_ref):
    length = qk_ref.shape[0]
    heads = state_ref.shape[0]
    key_dim = qk_ref.shape[1] // heads // 2
    value_dim = v_ref.shape[1] // heads
    scale = key_dim ** (-0.5)
    low = lax.broadcasted_iota(jnp.int32, (BLOCK, BLOCK), 0)
    high = lax.broadcasted_iota(jnp.int32, (BLOCK, BLOCK), 1)
    causal = high <= low
    states = [jnp.zeros((value_dim, key_dim), F32) for _ in range(heads)]
    for n in range(length // BLOCK):
        rows = slice(n * BLOCK, (n + 1) * BLOCK)
        for h in range(heads):
            keys = slice(h * key_dim, (h + 1) * key_dim)
            values = slice(h * value_dim, (h + 1) * value_dim)
            q = qk_ref[rows, keys].astype(F32) * scale
            k = qk_ref[rows, heads * key_dim + h * key_dim : heads * key_dim + (h + 1) * key_dim].astype(F32)
            v = v_ref[rows, values]
            qd = (q * in_ref[rows, keys]).astype(BF16)
            ki = (k * out_ref[rows, keys]).astype(BF16)
            kt = (k * tail_ref[rows, keys]).astype(BF16)
            qfar_ref[rows, keys] = (q * far_ref[rows, keys]).astype(BF16)
            scores = jnp.where(causal, across(qd, ki), 0.0).astype(BF16)
            part = dot(scores, v)
            if n > 0:
                part = part + across(qd, states[h].astype(BF16))
            part_ref[rows, values] = part
            update = lax.dot_general(v, kt, (((0,), (0,)), ((), ())), preferred_element_type=F32)
            states[h] = states[h] * end_ref[n : n + 1, keys] + update
    for h in range(heads):
        state_ref[h] = states[h]


def local_attention(qk, v, terms, heads):
    length, width = qk.shape[0], qk.shape[1] // 2
    wide = v.shape[1]
    return vmem_kernel(
        local_kernel,
        (
            jax.ShapeDtypeStruct((length, wide), F32),
            jax.ShapeDtypeStruct((length, width), BF16),
            jax.ShapeDtypeStruct((heads, wide // heads, width // heads), F32),
        ),
        6_000_000_000,
        qk,
        v,
        *terms,
        in_specs=[pl.BlockSpec(memory_space=pltpu.VMEM)] * (2 + len(terms)),
    )


def finish_kernel(part_ref, qfar_ref, state_ref, gain_ref, mixed_ref):
    heads = state_ref.shape[0]
    key_dim = qfar_ref.shape[1] // heads
    value_dim = part_ref.shape[1] // heads
    for h in range(heads):
        keys = slice(h * key_dim, (h + 1) * key_dim)
        values = slice(h * value_dim, (h + 1) * value_dim)
        attended = part_ref[:, values] + across(qfar_ref[:, keys], state_ref[h])
        meansq = jnp.mean(attended * attended, axis=-1, keepdims=True)
        gain = gain_ref[h : h + 1].astype(F32)
        mixed_ref[:, values] = (attended * lax.rsqrt(meansq + EPSILON) * gain).astype(BF16)


def finish_attention(part, qfar, state, gain):
    length, wide = part.shape
    return vmem_kernel(
        finish_kernel,
        jax.ShapeDtypeStruct((length, wide), BF16),
        3_000_000_000,
        part,
        qfar,
        state,
        gain,
        in_specs=[pl.BlockSpec(memory_space=pltpu.VMEM)] * 4,
    )


def unpack(packed, value_dim):
    packed = packed.astype(F32)
    return packed[:, value_dim : value_dim + 1], packed[:, :value_dim]


def combine(earlier, later):
    return earlier[0] * later[0], later[0] * earlier[1] + later[1]


def pack(pair):
    decay, state = pair
    heads, _, key_dim = state.shape
    lines = jnp.broadcast_to(decay, (heads, 16, key_dim))
    return jnp.concatenate([state, lines], axis=1).astype(BF16)


def entering(decay, state):
    value_dim = state.shape[1]
    z, y = lax.axis_index("z"), lax.axis_index("y")
    own = pack((decay, state))
    empty = (jnp.ones_like(decay), jnp.zeros_like(state))

    def only(passed, pair):
        return tuple(jnp.where(passed, a, b) for a, b in zip(pair, empty))

    before = empty
    total = (decay, state)
    got = [unpack(hop(own, "y", step), value_dim) for step in (1, 2, 3)]
    for step in (1, 2, 3):
        pair = got[step - 1]
        before = combine(only(y >= step, pair), before)
    after = empty
    for step in (3, 2, 1):
        after = combine(after, only(y < step, got[step - 1]))
    total = combine(combine(before, total), after)
    line = pack(total)
    outer = empty
    for step in (1, 2, 3):
        pair = unpack(onward(line, "z", step), value_dim)
        outer = combine(only(z >= step, pair), outer)
    return combine(outer, before)[1].astype(BF16)


def term_kernel(step, attn_ref, t_ref, b_ref, mixer_ref, filter_ref, own_ref, other_ref):
    x, c = lax.axis_index("x"), lax.axis_index("c")
    part = own_ref.shape[0]
    base = lax.rem(x + step, RING) * PAIR * part
    spots = [pl.multiple_of(base + core * part, HALO) for core in (1 - c, c)]
    half = t_ref.shape[1]
    out = None
    for ref, matrix in (
        (attn_ref, mixer_ref[...]),
        (t_ref, filter_ref[:half]),
        (b_ref, filter_ref[half:]),
    ):
        rows = jnp.concatenate([ref[pl.ds(at, part), :] for at in spots], axis=0)
        term = dot(rows, matrix)
        out = term if out is None else out + term
    other_ref[...] = out[:part].astype(BF16)
    own_ref[...] = out[part:]


def term_call(step, attn, t, b, mixer, filt, part):
    width = mixer.shape[1]
    tile = 1024
    whole = pl.BlockSpec(memory_space=pltpu.VMEM)
    return vmem_kernel(
        functools.partial(term_kernel, step),
        (
            jax.ShapeDtypeStruct((part, width), F32),
            jax.ShapeDtypeStruct((part, width), BF16),
        ),
        2_000_000_000,
        attn,
        t,
        b,
        mixer,
        filt,
        grid=(width // tile,),
        in_specs=[whole, whole, whole]
        + [pl.BlockSpec((m.shape[0], tile), lambda i: (0, i)) for m in (mixer, filt)],
        out_specs=(
            pl.BlockSpec((part, tile), lambda i: (0, i)),
            pl.BlockSpec((part, tile), lambda i: (0, i)),
        ),
    )


def plus(*terms):
    total = terms[0].astype(F32)
    for term in terms[1:]:
        total = total + term.astype(F32)
    return total


def body(
    hidden,
    entry_gain,
    probe,
    lookup,
    payload,
    postfilter,
    prefilter,
    source,
    forget_left,
    forget_right,
    forget_offset,
    forget_spike,
    head_gain,
    taps,
    mixer_result,
    filter_result,
):
    heads, value_dim = head_gain.shape
    key_dim = probe.shape[1] // heads
    channels = taps.shape[1]
    half = channels // 2
    keys, values = 2 * heads * key_dim, heads * value_dim

    def shard(attn, cols):
        convs = [w[:, cols] for w in (postfilter, prefilter, source)]
        return jnp.concatenate(attn + convs, axis=1)

    tops = shard([probe, lookup], slice(0, half))
    bottoms = shard([payload], slice(half, channels))
    first = around(tops, "z")
    second = around(bottoms, "y")
    normed = norm_values(hidden, entry_gain).astype(BF16)
    part = normed.shape[0]
    rim = onward(normed[part - HALO :], SP, 1)
    x = gather_rows(jnp.concatenate([normed, rim], axis=0))

    line_qk, line_t = line_up("z", first, (keys, 3 * half))
    line_v, line_b = line_up("y", second, (values, 3 * half))
    w_qk = around(line_qk, "y")
    w_v = around(line_v, "z")
    w_t = around(line_t, "y")
    w_b = around(line_b, "z")

    *terms, total = decay_terms(x, forget_left, forget_right, forget_offset, forget_spike)
    total = total.reshape(heads, 1, key_dim)
    early, late = (0, 1, 2), (3, 4)
    acc_qk = project_call(x, None, w_qk[:3], early, 1, HALO, F32)
    acc_v = project_call(x, None, w_v[:3], early, 0, HALO, F32)
    qk = project_call(x, acc_qk, w_qk[3:], late, 1, HALO, BF16)
    v = project_call(x, acc_v, w_v[3:], late, 0, HALO, BF16)
    near, qfar, state = local_attention(qk, v, terms, heads)
    incoming = entering(total, state)
    mixed_attn = finish_attention(near, qfar, incoming, head_gain)

    acc_t = project_call(x, None, w_t[:3], early, 1, 0, F32)
    acc_b = project_call(x, None, w_b[:3], early, 0, 0, F32)
    mixed_t = gate_call(x, acc_t, w_t[3:], late, taps[:, :half], 1)
    mixed_b = gate_call(x, acc_b, w_b[3:], late, taps[:, half:], 0)

    def partial(step):
        own, other = term_call(
            step, mixed_attn, mixed_t, mixed_b, mixer_result, filter_result, part
        )
        return plus(own, swap(other))

    cut = part // 2
    far = partial(2).astype(BF16)
    far_up, far_down = hop(far[:cut], "x", 1), hop(far[cut:], "x", -1)
    up, down = partial(1), partial(3)
    plain_up = hop(up[cut:].astype(BF16), "x", 1)
    plain_down = hop(down[:cut].astype(BF16), "x", -1)
    last_up = hop(plus(up[:cut], far_up).astype(BF16), "x", 1)
    last_down = hop(plus(down[cut:], far_down).astype(BF16), "x", -1)
    from_below = jnp.concatenate([last_up, plain_up], axis=0)
    from_above = jnp.concatenate([plain_down, last_down], axis=0)
    return plus(partial(0), from_below, from_above).astype(BF16)


def solution(mesh):
    split = Mesh(mesh.devices.reshape(RING, RING, RING, PAIR), ALL)
    in_specs = (
        P(ALL, None),
        P(),
        P(SP, TP),
        P(SP, TP),
        P(SP, TP),
        P(SP, TP),
        P(SP, TP),
        P(SP, TP),
        P(),
        P(None, TP),
        P(TP),
        P(TP, SP),
        P(TP, None),
        P(None, TP),
        P(TP, None),
        P(TP, None),
    )

    return jax.shard_map(
        body, mesh=split, in_specs=in_specs, out_specs=P(ALL, None), check_vma=False
    )
```

```python
import functools

import jax
import jax.numpy as jnp
from jax import lax
from jax.experimental import pallas as pl
from jax.experimental.pallas import tpu as pltpu
from jax.sharding import Mesh
from jax.sharding import PartitionSpec as P

BLOCK = 64
SP = ("z", "y")
TP = ("x", "c")
ALL = ("z", "y", "x", "c")
RING = 4
PAIR = 2
HALO = 16

EPSILON = 1e-06
SOFTNESS = 16.0

F32 = jnp.float32
BF16 = jnp.bfloat16


def dot(a, b):
    return jnp.dot(a, b, preferred_element_type=F32)


def hop(value, axis, steps):
    return lax.ppermute(value, axis, [(i, (i + steps) % RING) for i in range(RING)])


def swap(value):
    return lax.ppermute(value, "c", [(0, 1), (1, 0)])


def onward(value, axis, steps):
    count = RING * RING if axis == SP else RING
    return lax.ppermute(value, axis, [(i, i + steps) for i in range(count - steps)])


def around(value, axis, half=None):
    half = half or value.shape[0] // 2
    below, above = hop(value, axis, 1), hop(value, axis, -1)
    top = hop(below[:half], axis, 1)
    bottom = hop(above[half:], axis, -1)
    return value, below, above, top, bottom


def vmem_kernel(kernel, out_shape, flops, *args, **kwargs):
    return pl.pallas_call(
        kernel,
        out_shape=out_shape,
        compiler_params=pltpu.CompilerParams(vmem_limit_bytes=kwargs.pop("limit", 16) << 20),
        cost_estimate=pl.CostEstimate(
            flops=flops, bytes_accessed=8_000_000, transcendentals=0
        ),
        **kwargs,
    )(*args)


def line_kernel(axis, own, below, above, top, bottom, *outs):
    me = lax.axis_index(axis)
    rows = own.shape[0]
    half = rows // 2
    at = 0
    for out in outs:
        cols = slice(at, at + out.shape[1])
        at += out.shape[1]
        for ref, step, offset in (
            (own, 0, 0),
            (below, 3, 0),
            (above, 1, 0),
            (top, 2, 0),
            (bottom, 2, half),
        ):
            start = pl.multiple_of(lax.rem(me + step, RING) * rows + offset, half)
            out[pl.ds(start, ref.shape[0]), :] = ref[:, cols]


def line_up(axis, pieces, widths):
    rows = pieces[0].shape[0] * RING
    return vmem_kernel(
        functools.partial(line_kernel, axis),
        tuple(jax.ShapeDtypeStruct((rows, w), BF16) for w in widths),
        1_000_000_000,
        *pieces,
    )


def chips_kernel(own, below, above, top, bottom, out):
    x = lax.axis_index("x")
    rows = own.shape[0]
    half = top.shape[0]
    for ref, step, offset in (
        (own, 0, 0),
        (below, 3, 0),
        (above, 1, 0),
        (top, 2, 0),
        (bottom, 2, half),
    ):
        start = pl.multiple_of(lax.rem(x + step, RING) * rows + offset, HALO)
        out[pl.ds(start, ref.shape[0]), :] = ref[...]


def rows_kernel(mine, other, out):
    c = lax.axis_index("c")
    block = mine.shape[0] // RING
    part = block - HALO
    for ref, core in ((mine, c), (other, 1 - c)):
        for chip in range(RING):
            start = pl.multiple_of(HALO + (chip * PAIR + core) * part, HALO)
            out[pl.ds(start, part), :] = ref[chip * block : chip * block + part]

        @pl.when(core == 1)
        def _(ref=ref):
            out[:HALO] = ref[RING * block - HALO :]


def gather_rows(shard):
    block, width = shard.shape
    part = block - HALO
    pieces = around(shard, "x", part // 2)
    mine = vmem_kernel(
        chips_kernel, jax.ShapeDtypeStruct((RING * block, width), BF16), 1_000_000_000, *pieces
    )
    return vmem_kernel(
        rows_kernel,
        jax.ShapeDtypeStruct((HALO + RING * PAIR * part, width), BF16),
        2_000_000_000,
        mine,
        swap(mine),
    )


def project(x_ref, lead, along, pieces, which, block):
    me = lax.axis_index("z" if along == 0 else "y")
    total = None
    for ref, index in zip(pieces, which):
        step, first = ((0, 0), (3, 0), (1, 0), (2, 0), (2, 2))[index]
        where = lax.rem(me + step, RING)
        count = ref.shape[0] // block
        if along == 0:
            start = pl.multiple_of((where * RING + first) * block, block)
            term = dot(x_ref[lead:, pl.ds(start, count * block)], ref[...])
            total = term if total is None else total + term
        else:
            for i in range(count):
                start = pl.multiple_of(((first + i) * RING + where) * block, block)
                term = dot(
                    x_ref[lead:, pl.ds(start, block)], ref[i * block : (i + 1) * block, :]
                )
                total = term if total is None else total + term
    return total


def project_kernel(lead, along, which, block, x_ref, *refs):
    *pieces, out = refs
    out[...] = project(x_ref, lead, along, pieces, which, block).astype(out.dtype)


def project_more_kernel(lead, along, which, block, x_ref, acc_ref, *refs):
    *pieces, out = refs
    total = acc_ref[...] + project(x_ref, lead, along, pieces, which, block)
    out[...] = total.astype(out.dtype)


def project_call(x, acc, pieces, which, along, lead, dtype, tile=256):
    block = x.shape[1] // (RING * RING)
    rows = x.shape[0] - lead
    width = pieces[0].shape[1]
    more = () if acc is None else (acc,)
    kernel = project_kernel if acc is None else project_more_kernel
    return vmem_kernel(
        functools.partial(kernel, lead, along, which, block),
        jax.ShapeDtypeStruct((rows, width), dtype),
        3_000_000_000,
        x,
        *more,
        *pieces,
        grid=(width // tile,),
        in_specs=[pl.BlockSpec(memory_space=pltpu.VMEM)]
        + [pl.BlockSpec((rows, tile), lambda i: (0, i)) for _ in more]
        + [pl.BlockSpec((p.shape[0], tile), lambda i: (0, i)) for p in pieces],
        out_specs=pl.BlockSpec((rows, tile), lambda i: (0, i)),
    )


def gate_kernel(along, which, block, x_ref, acc_ref, *refs):
    *pieces, taps_ref, out = refs
    sums = (acc_ref[...] + project(x_ref, 0, along, pieces, which, block)).astype(BF16)
    width = sums.shape[1] // 3
    length = sums.shape[0] - HALO
    gated = (sums[:, width : 2 * width].astype(F32) * sums[:, 2 * width :].astype(F32)).astype(BF16)
    gated = gated.astype(F32)
    taps = taps_ref.shape[0]
    conv = jnp.zeros((length, width), F32)
    for i in range(taps):
        lead = HALO + 1 - taps + i
        conv = conv + taps_ref[i : i + 1, :].astype(F32) * gated[lead : lead + length]
    out[...] = (conv * sums[HALO:, :width].astype(F32)).astype(BF16)


def gate_call(x, acc, pieces, which, taps, along):
    block = x.shape[1] // (RING * RING)
    return vmem_kernel(
        functools.partial(gate_kernel, along, which, block),
        jax.ShapeDtypeStruct((x.shape[0] - HALO, taps.shape[1]), BF16),
        2_000_000_000,
        x,
        acc,
        *pieces,
        taps,
        in_specs=[pl.BlockSpec(memory_space=pltpu.VMEM)] * (3 + len(pieces)),
        out_specs=pl.BlockSpec(memory_space=pltpu.VMEM),
    )


def norm_kernel(rows_ref, gain_ref, out_ref):
    rows = rows_ref[...].astype(F32)
    meansq = jnp.mean(rows * rows, axis=-1, keepdims=True)
    normed = rows * lax.rsqrt(meansq + EPSILON) * gain_ref[...].astype(F32)
    out_ref[...] = normed.astype(BF16)


def norm_rows(rows, gain):
    return vmem_kernel(
        norm_kernel, jax.ShapeDtypeStruct(rows.shape, BF16), 1_000_000, rows, gain[None]
    )


def decay_kernel(
    x_ref, left_ref, right_ref, offset_ref, spike_ref, in_ref, out_ref, tail_ref, far_ref, end_ref, total_ref
):
    length, width = in_ref.shape
    heads = spike_ref.shape[0]
    low_rank = across(x_ref[HALO:, :], left_ref[...]).astype(BF16)
    gate = dot(low_rank, right_ref[...]) + offset_ref[...]
    soft = jnp.minimum(gate, 0.0) - jnp.log1p(jnp.exp(-jnp.abs(gate)))
    head = lax.broadcasted_iota(jnp.int32, (heads, width), 0)
    feature = lax.broadcasted_iota(jnp.int32, (heads, width), 1)
    owner = jnp.where(feature // (width // heads) == head, 1.0, 0.0).astype(F32)
    spikes = lax.dot_general(
        spike_ref[...],
        owner,
        (((0,), (0,)), ((), ())),
        preferred_element_type=F32,
        precision=lax.Precision.HIGHEST,
    )
    rate = soft / SOFTNESS + spikes
    low = lax.broadcasted_iota(jnp.int32, (BLOCK, BLOCK), 0)
    high = lax.broadcasted_iota(jnp.int32, (BLOCK, BLOCK), 1)
    tri = jnp.where(high <= low, 1.0, 0.0).astype(F32)
    prefix = jnp.zeros((1, width), F32)
    tail_ref[...] = rate

    def step(n, prefix):
        rows = pl.ds(pl.multiple_of(n * BLOCK, BLOCK), BLOCK)
        within = jnp.dot(
            tri, tail_ref[rows, :], preferred_element_type=F32, precision=lax.Precision.HIGHEST
        )
        end = within[BLOCK - 1 :]
        grow = jnp.exp(within)
        in_ref[rows, :] = grow
        out_ref[rows, :] = jnp.exp(-within)
        tail_ref[rows, :] = jnp.exp(end - within)
        far_ref[rows, :] = grow * jnp.exp(prefix)
        end_ref[pl.ds(n, 1), :] = jnp.exp(end)
        return prefix + end

    total_ref[...] = jnp.exp(lax.fori_loop(0, length // BLOCK, step, prefix))


def decay_terms(x, left, right, offset, spike):
    length, width = x.shape[0] - HALO, right.shape[1]
    full = jax.ShapeDtypeStruct((length, width), F32)
    return vmem_kernel(
        decay_kernel,
        (
            full,
            full,
            full,
            full,
            jax.ShapeDtypeStruct((length // BLOCK, width), F32),
            jax.ShapeDtypeStruct((1, width), F32),
        ),
        4_000_000_000,
        x,
        jnp.transpose(left),
        right,
        offset[None],
        spike,
        in_specs=[pl.BlockSpec(memory_space=pltpu.VMEM)] * 5,
    )


def across(a, b):
    return lax.dot_general(a, b, (((1,), (1,)), ((), ())), preferred_element_type=F32)


def local_kernel(qk_ref, v_ref, in_ref, out_ref, tail_ref, far_ref, end_ref, part_ref, qfar_ref, state_ref):
    length = qk_ref.shape[0]
    heads = state_ref.shape[0]
    key_dim = qk_ref.shape[1] // heads // 2
    value_dim = v_ref.shape[1] // heads
    scale = key_dim ** (-0.5)
    low = lax.broadcasted_iota(jnp.int32, (BLOCK, BLOCK), 0)
    high = lax.broadcasted_iota(jnp.int32, (BLOCK, BLOCK), 1)
    causal = high <= low
    states = [jnp.zeros((value_dim, key_dim), F32) for _ in range(heads)]
    for n in range(length // BLOCK):
        rows = slice(n * BLOCK, (n + 1) * BLOCK)
        for h in range(heads):
            keys = slice(h * key_dim, (h + 1) * key_dim)
            values = slice(h * value_dim, (h + 1) * value_dim)
            q = qk_ref[rows, keys].astype(F32) * scale
            k = qk_ref[rows, heads * key_dim + h * key_dim : heads * key_dim + (h + 1) * key_dim].astype(F32)
            v = v_ref[rows, values]
            qd = (q * in_ref[rows, keys]).astype(BF16)
            ki = (k * out_ref[rows, keys]).astype(BF16)
            kt = (k * tail_ref[rows, keys]).astype(BF16)
            qfar_ref[rows, keys] = (q * far_ref[rows, keys]).astype(BF16)
            scores = jnp.where(causal, across(qd, ki), 0.0).astype(BF16)
            part = dot(scores, v)
            if n > 0:
                part = part + across(qd, states[h].astype(BF16))
            part_ref[rows, values] = part
            update = lax.dot_general(v, kt, (((0,), (0,)), ((), ())), preferred_element_type=F32)
            states[h] = states[h] * end_ref[n : n + 1, keys] + update
    for h in range(heads):
        state_ref[h] = states[h]


def local_attention(qk, v, terms, heads):
    length, width = qk.shape[0], qk.shape[1] // 2
    wide = v.shape[1]
    return vmem_kernel(
        local_kernel,
        (
            jax.ShapeDtypeStruct((length, wide), F32),
            jax.ShapeDtypeStruct((length, width), BF16),
            jax.ShapeDtypeStruct((heads, wide // heads, width // heads), F32),
        ),
        6_000_000_000,
        qk,
        v,
        *terms,
        in_specs=[pl.BlockSpec(memory_space=pltpu.VMEM)] * (2 + len(terms)),
    )


def finish_kernel(part_ref, qfar_ref, state_ref, gain_ref, mixed_ref):
    heads = state_ref.shape[0]
    key_dim = qfar_ref.shape[1] // heads
    value_dim = part_ref.shape[1] // heads
    for h in range(heads):
        keys = slice(h * key_dim, (h + 1) * key_dim)
        values = slice(h * value_dim, (h + 1) * value_dim)
        attended = part_ref[:, values] + across(qfar_ref[:, keys], state_ref[h])
        meansq = jnp.mean(attended * attended, axis=-1, keepdims=True)
        gain = gain_ref[h : h + 1].astype(F32)
        mixed_ref[:, values] = (attended * lax.rsqrt(meansq + EPSILON) * gain).astype(BF16)


def finish_attention(part, qfar, state, gain):
    length, wide = part.shape
    return vmem_kernel(
        finish_kernel,
        jax.ShapeDtypeStruct((length, wide), BF16),
        100_000_000,
        part,
        qfar,
        state,
        gain,
        in_specs=[pl.BlockSpec(memory_space=pltpu.VMEM)] * 4,
    )


def unpack(packed, value_dim):
    packed = packed.astype(F32)
    return packed[:, value_dim : value_dim + 1], packed[:, :value_dim]


def combine(earlier, later):
    return earlier[0] * later[0], later[0] * earlier[1] + later[1]


def pack(pair):
    decay, state = pair
    heads, _, key_dim = state.shape
    lines = jnp.broadcast_to(decay, (heads, 16, key_dim))
    return jnp.concatenate([state, lines], axis=1).astype(BF16)


def entering(decay, state):
    value_dim = state.shape[1]
    z, y = lax.axis_index("z"), lax.axis_index("y")
    own = pack((decay, state))
    empty = (jnp.ones_like(decay), jnp.zeros_like(state))

    def only(passed, pair):
        return tuple(jnp.where(passed, a, b) for a, b in zip(pair, empty))

    before = empty
    total = (decay, state)
    got = [unpack(hop(own, "y", step), value_dim) for step in (1, 2, 3)]
    for step in (1, 2, 3):
        pair = got[step - 1]
        before = combine(only(y >= step, pair), before)
    after = empty
    for step in (3, 2, 1):
        after = combine(after, only(y < step, got[step - 1]))
    total = combine(combine(before, total), after)
    line = pack(total)
    outer = empty
    for step in (1, 2, 3):
        pair = unpack(onward(line, "z", step), value_dim)
        outer = combine(only(z >= step, pair), outer)
    return combine(outer, before)[1].astype(BF16)


def term_kernel(steps, attn_ref, t_ref, b_ref, mixer_ref, filter_ref, own_ref, other_ref):
    x, c = lax.axis_index("x"), lax.axis_index("c")
    count = own_ref.shape[0]
    part = count // len(steps)
    spots = [
        pl.multiple_of((lax.rem(x + step, RING) * PAIR + core) * part, HALO)
        for core in (1 - c, c)
        for step in steps
    ]
    half = t_ref.shape[1]
    out = None
    for ref, matrix in (
        (attn_ref, mixer_ref[...]),
        (t_ref, filter_ref[:half]),
        (b_ref, filter_ref[half:]),
    ):
        rows = jnp.concatenate([ref[pl.ds(at, part), :] for at in spots], axis=0)
        term = dot(rows, matrix)
        out = term if out is None else out + term
    other_ref[...] = out[:count].astype(BF16)
    own_ref[...] = out[count:]


def term_call(steps, attn, t, b, mixer, filt, part):
    width = mixer.shape[1]
    part = part * len(steps)
    tile = 1024
    whole = pl.BlockSpec(memory_space=pltpu.VMEM)
    return vmem_kernel(
        functools.partial(term_kernel, steps),
        (
            jax.ShapeDtypeStruct((part, width), F32),
            jax.ShapeDtypeStruct((part, width), BF16),
        ),
        2_000_000_000,
        attn,
        t,
        b,
        mixer,
        filt,
        grid=(width // tile,),
        in_specs=[whole, whole, whole]
        + [pl.BlockSpec((m.shape[0], tile), lambda i: (0, i)) for m in (mixer, filt)],
        out_specs=(
            pl.BlockSpec((part, tile), lambda i: (0, i)),
            pl.BlockSpec((part, tile), lambda i: (0, i)),
        ),
    )


def plus(*terms):
    total = terms[0].astype(F32)
    for term in terms[1:]:
        total = total + term.astype(F32)
    return total


def body(
    hidden,
    entry_gain,
    probe,
    lookup,
    payload,
    postfilter,
    prefilter,
    source,
    forget_left,
    forget_right,
    forget_offset,
    forget_spike,
    head_gain,
    taps,
    mixer_result,
    filter_result,
):
    heads, value_dim = head_gain.shape
    key_dim = probe.shape[1] // heads
    channels = taps.shape[1]
    half = channels // 2
    keys, values = 2 * heads * key_dim, heads * value_dim

    def shard(attn, convs, cols):
        return jnp.concatenate(attn + [w[:, cols] for w in convs], axis=1)

    normed = norm_rows(hidden, entry_gain)
    part = normed.shape[0]
    rim = onward(normed[part - HALO :], SP, 1)
    convs = (postfilter, prefilter, source)
    tops = shard([probe, lookup], convs, slice(0, half))
    bottoms = shard([payload], lax.optimization_barrier(convs), slice(half, channels))
    first = around(tops, "z")
    second = around(bottoms, "y")
    x = gather_rows(jnp.concatenate([normed, rim], axis=0))

    line_qk, line_t = line_up("z", first, (keys, 3 * half))
    line_v, line_b = line_up("y", second, (values, 3 * half))
    w_qk = around(line_qk, "y")
    w_v = around(line_v, "z")
    w_t = around(line_t, "y")
    w_b = around(line_b, "z")

    *terms, total = decay_terms(x, forget_left, forget_right, forget_offset, forget_spike)
    total = total.reshape(heads, 1, key_dim)
    early, late = (0, 1, 2), (3, 4)
    acc_qk = project_call(x, None, w_qk[:3], early, 1, HALO, F32)
    acc_v = project_call(x, None, w_v[:3], early, 0, HALO, F32)
    qk = project_call(x, acc_qk, w_qk[3:], late, 1, HALO, BF16)
    v = project_call(x, acc_v, w_v[3:], late, 0, HALO, BF16)
    near, qfar, state = local_attention(qk, v, terms, heads)
    incoming = entering(total, state)
    mixed_attn = finish_attention(near, qfar, incoming, head_gain)

    acc_t = project_call(x, None, w_t[:3], early, 1, 0, F32)
    acc_b = project_call(x, None, w_b[:3], early, 0, 0, F32)
    mixed_t = gate_call(x, acc_t, w_t[3:], late, taps[:, :half], 1)
    mixed_b = gate_call(x, acc_b, w_b[3:], late, taps[:, half:], 0)

    def partial(*steps):
        own, other = term_call(
            steps, mixed_attn, mixed_t, mixed_b, mixer_result, filter_result, part
        )
        return plus(own, swap(other))

    cut = part // 2
    far = partial(2).astype(BF16)
    far_up, far_down = hop(far[:cut], "x", 1), hop(far[cut:], "x", -1)
    near_terms = partial(1, 3)
    up, down = near_terms[:part], near_terms[part:]
    plain_up = hop(up[cut:].astype(BF16), "x", 1)
    plain_down = hop(down[:cut].astype(BF16), "x", -1)
    last_up = hop(plus(up[:cut], far_up).astype(BF16), "x", 1)
    last_down = hop(plus(down[cut:], far_down).astype(BF16), "x", -1)
    from_below = jnp.concatenate([last_up, plain_up], axis=0)
    from_above = jnp.concatenate([plain_down, last_down], axis=0)
    return plus(partial(0), from_below, from_above).astype(BF16)


def solution(mesh):
    split = Mesh(mesh.devices.reshape(RING, RING, RING, PAIR), ALL)
    in_specs = (
        P(ALL, None),
        P(),
        P(SP, TP),
        P(SP, TP),
        P(SP, TP),
        P(SP, TP),
        P(SP, TP),
        P(SP, TP),
        P(),
        P(None, TP),
        P(TP),
        P(TP, SP),
        P(TP, None),
        P(None, TP),
        P(TP, None),
        P(TP, None),
    )

    return jax.shard_map(
        body, mesh=split, in_specs=in_specs, out_specs=P(ALL, None), check_vma=False
    )
```

```python
import functools

import jax
import jax.numpy as jnp
from jax import lax
from jax.experimental import pallas as pl
from jax.experimental.pallas import tpu as pltpu
from jax.sharding import Mesh
from jax.sharding import PartitionSpec as P

BLOCK = 64
SP = ("z", "y")
TP = ("x", "c")
ALL = ("z", "y", "x", "c")
RING = 4
PAIR = 2
HALO = 16

EPSILON = 1e-06
SOFTNESS = 16.0

F32 = jnp.float32
BF16 = jnp.bfloat16


def dot(a, b):
    return jnp.dot(a, b, preferred_element_type=F32)


def hop(value, axis, steps):
    return lax.ppermute(value, axis, [(i, (i + steps) % RING) for i in range(RING)])


def swap(value):
    return lax.ppermute(value, "c", [(0, 1), (1, 0)])


def onward(value, axis, steps):
    count = RING * RING if axis == SP else RING
    return lax.ppermute(value, axis, [(i, i + steps) for i in range(count - steps)])


def around(value, axis, half=None):
    half = half or value.shape[0] // 2
    below, above = hop(value, axis, 1), hop(value, axis, -1)
    top = hop(below[:half], axis, 1)
    bottom = hop(above[half:], axis, -1)
    return value, below, above, top, bottom


def vmem_kernel(kernel, out_shape, flops, *args, **kwargs):
    return pl.pallas_call(
        kernel,
        out_shape=out_shape,
        compiler_params=pltpu.CompilerParams(vmem_limit_bytes=kwargs.pop("limit", 10) << 20),
        cost_estimate=pl.CostEstimate(
            flops=flops, bytes_accessed=8_000_000, transcendentals=0
        ),
        **kwargs,
    )(*args)


def line_kernel(axis, own, below, above, top, bottom, *outs):
    me = lax.axis_index(axis)
    rows = own.shape[0]
    half = rows // 2
    at = 0
    for out in outs:
        cols = slice(at, at + out.shape[1])
        at += out.shape[1]
        for ref, step, offset in (
            (own, 0, 0),
            (below, 3, 0),
            (above, 1, 0),
            (top, 2, 0),
            (bottom, 2, half),
        ):
            start = pl.multiple_of(lax.rem(me + step, RING) * rows + offset, half)
            out[pl.ds(start, ref.shape[0]), :] = ref[:, cols]


def line_up(axis, pieces, widths):
    rows = pieces[0].shape[0] * RING
    return vmem_kernel(
        functools.partial(line_kernel, axis),
        tuple(jax.ShapeDtypeStruct((rows, w), BF16) for w in widths),
        1_000_000_000,
        *pieces,
    )


def chips_kernel(own, below, above, top, bottom, out):
    x = lax.axis_index("x")
    rows = own.shape[0]
    half = top.shape[0]
    for ref, step, offset in (
        (own, 0, 0),
        (below, 3, 0),
        (above, 1, 0),
        (top, 2, 0),
        (bottom, 2, half),
    ):
        start = pl.multiple_of(lax.rem(x + step, RING) * rows + offset, HALO)
        out[pl.ds(start, ref.shape[0]), :] = ref[...]


def rows_kernel(mine, other, out):
    c = lax.axis_index("c")
    block = mine.shape[0] // RING
    part = block - HALO
    for ref, core in ((mine, c), (other, 1 - c)):
        for chip in range(RING):
            start = pl.multiple_of(HALO + (chip * PAIR + core) * part, HALO)
            out[pl.ds(start, part), :] = ref[chip * block : chip * block + part]

        @pl.when(core == 1)
        def _(ref=ref):
            out[:HALO] = ref[RING * block - HALO :]


def gather_rows(shard):
    block, width = shard.shape
    part = block - HALO
    pieces = around(shard, "x", part // 2)
    mine = vmem_kernel(
        chips_kernel,
        jax.ShapeDtypeStruct((RING * block, width), BF16),
        1_000_000_000,
        *pieces,
        limit=16,
    )
    return vmem_kernel(
        rows_kernel,
        jax.ShapeDtypeStruct((HALO + RING * PAIR * part, width), BF16),
        2_000_000_000,
        mine,
        swap(mine),
        limit=16,
    )


def project(x_ref, lead, along, pieces, which, block):
    me = lax.axis_index("z" if along == 0 else "y")
    total = None
    for ref, index in zip(pieces, which):
        step, first = ((0, 0), (3, 0), (1, 0), (2, 0), (2, 2))[index]
        where = lax.rem(me + step, RING)
        count = ref.shape[0] // block
        if along == 0:
            start = pl.multiple_of((where * RING + first) * block, block)
            term = dot(x_ref[lead:, pl.ds(start, count * block)], ref[...])
            total = term if total is None else total + term
        else:
            for i in range(count):
                start = pl.multiple_of(((first + i) * RING + where) * block, block)
                term = dot(
                    x_ref[lead:, pl.ds(start, block)], ref[i * block : (i + 1) * block, :]
                )
                total = term if total is None else total + term
    return total


def project_kernel(lead, along, which, block, x_ref, *refs):
    *pieces, out = refs
    out[...] = project(x_ref, lead, along, pieces, which, block).astype(out.dtype)


def project_more_kernel(lead, along, which, block, x_ref, acc_ref, *refs):
    *pieces, out = refs
    total = acc_ref[...] + project(x_ref, lead, along, pieces, which, block)
    out[...] = total.astype(out.dtype)


def project_call(x, acc, pieces, which, along, lead, dtype, tile=256):
    block = x.shape[1] // (RING * RING)
    rows = x.shape[0] - lead
    width = pieces[0].shape[1]
    more = () if acc is None else (acc,)
    kernel = project_kernel if acc is None else project_more_kernel
    return vmem_kernel(
        functools.partial(kernel, lead, along, which, block),
        jax.ShapeDtypeStruct((rows, width), dtype),
        3_000_000_000,
        x,
        *more,
        *pieces,
        grid=(width // tile,),
        in_specs=[pl.BlockSpec(memory_space=pltpu.VMEM)]
        + [pl.BlockSpec((rows, tile), lambda i: (0, i)) for _ in more]
        + [pl.BlockSpec((p.shape[0], tile), lambda i: (0, i)) for p in pieces],
        out_specs=pl.BlockSpec((rows, tile), lambda i: (0, i)),
    )


def gate_kernel(along, which, block, x_ref, acc_ref, *refs):
    *pieces, taps_ref, out = refs
    sums = (acc_ref[...] + project(x_ref, 0, along, pieces, which, block)).astype(BF16)
    width = sums.shape[1] // 3
    length = sums.shape[0] - HALO
    gated = (sums[:, width : 2 * width].astype(F32) * sums[:, 2 * width :].astype(F32)).astype(BF16)
    gated = gated.astype(F32)
    taps = taps_ref.shape[0]
    conv = jnp.zeros((length, width), F32)
    for i in range(taps):
        lead = HALO + 1 - taps + i
        conv = conv + taps_ref[i : i + 1, :].astype(F32) * gated[lead : lead + length]
    out[...] = (conv * sums[HALO:, :width].astype(F32)).astype(BF16)


def gate_call(x, acc, pieces, which, taps, along):
    block = x.shape[1] // (RING * RING)
    return vmem_kernel(
        functools.partial(gate_kernel, along, which, block),
        jax.ShapeDtypeStruct((x.shape[0] - HALO, taps.shape[1]), BF16),
        2_000_000_000,
        x,
        acc,
        *pieces,
        taps,
        in_specs=[pl.BlockSpec(memory_space=pltpu.VMEM)] * (3 + len(pieces)),
        out_specs=pl.BlockSpec(memory_space=pltpu.VMEM),
    )


def norm_kernel(rows_ref, gain_ref, out_ref):
    rows = rows_ref[...].astype(F32)
    meansq = jnp.mean(rows * rows, axis=-1, keepdims=True)
    normed = rows * lax.rsqrt(meansq + EPSILON) * gain_ref[...].astype(F32)[None]
    out_ref[...] = normed.astype(BF16)


def norm_rows(rows, gain):
    return vmem_kernel(norm_kernel, jax.ShapeDtypeStruct(rows.shape, BF16), 1_000_000, rows, gain)


def decay_kernel(
    x_ref, left_ref, right_ref, offset_ref, spike_ref, in_ref, out_ref, tail_ref, far_ref, end_ref, total_ref
):
    length, width = in_ref.shape
    heads = spike_ref.shape[0]
    low_rank = across(x_ref[HALO:, :], left_ref[...]).astype(BF16)
    gate = dot(low_rank, right_ref[...]) + offset_ref[...]
    soft = jnp.minimum(gate, 0.0) - jnp.log1p(jnp.exp(-jnp.abs(gate)))
    head = lax.broadcasted_iota(jnp.int32, (heads, width), 0)
    feature = lax.broadcasted_iota(jnp.int32, (heads, width), 1)
    owner = jnp.where(feature // (width // heads) == head, 1.0, 0.0).astype(F32)
    spikes = lax.dot_general(
        spike_ref[...],
        owner,
        (((0,), (0,)), ((), ())),
        preferred_element_type=F32,
        precision=lax.Precision.HIGHEST,
    )
    rate = soft / SOFTNESS + spikes
    low = lax.broadcasted_iota(jnp.int32, (BLOCK, BLOCK), 0)
    high = lax.broadcasted_iota(jnp.int32, (BLOCK, BLOCK), 1)
    tri = jnp.where(high <= low, 1.0, 0.0).astype(F32)
    prefix = jnp.zeros((1, width), F32)
    tail_ref[...] = rate

    def step(n, prefix):
        rows = pl.ds(pl.multiple_of(n * BLOCK, BLOCK), BLOCK)
        within = jnp.dot(
            tri, tail_ref[rows, :], preferred_element_type=F32, precision=lax.Precision.HIGHEST
        )
        end = within[BLOCK - 1 :]
        grow = jnp.exp(within)
        in_ref[rows, :] = grow
        out_ref[rows, :] = jnp.exp(-within)
        tail_ref[rows, :] = jnp.exp(end - within)
        far_ref[rows, :] = grow * jnp.exp(prefix)
        end_ref[pl.ds(n, 1), :] = jnp.exp(end)
        return prefix + end

    total_ref[...] = jnp.exp(lax.fori_loop(0, length // BLOCK, step, prefix))


def decay_terms(x, left, right, offset, spike):
    length, width = x.shape[0] - HALO, right.shape[1]
    full = jax.ShapeDtypeStruct((length, width), F32)
    return vmem_kernel(
        decay_kernel,
        (
            full,
            full,
            full,
            full,
            jax.ShapeDtypeStruct((length // BLOCK, width), F32),
            jax.ShapeDtypeStruct((1, width), F32),
        ),
        4_000_000_000,
        x,
        jnp.transpose(left),
        right,
        offset[None],
        spike,
        in_specs=[pl.BlockSpec(memory_space=pltpu.VMEM)] * 5,
    )


def across(a, b):
    return lax.dot_general(a, b, (((1,), (1,)), ((), ())), preferred_element_type=F32)


def state_kernel(qk_ref, v_ref, tail_ref, end_ref, enter_ref, state_ref):
    heads, value_dim, key_dim = state_ref.shape
    for h in range(heads):
        keys = slice(h * key_dim, (h + 1) * key_dim)
        lanes = slice((heads + h) * key_dim, (heads + h + 1) * key_dim)
        values = slice(h * value_dim, (h + 1) * value_dim)
        state = jnp.zeros((value_dim, key_dim), F32)
        for n in range(v_ref.shape[0] // BLOCK):
            rows = slice(n * BLOCK, (n + 1) * BLOCK)
            enter_ref[n, h] = state.astype(BF16)
            kt = (qk_ref[rows, lanes].astype(F32) * tail_ref[rows, keys]).astype(BF16)
            update = lax.dot_general(
                v_ref[rows, values], kt, (((0,), (0,)), ((), ())), preferred_element_type=F32
            )
            state = state * end_ref[n : n + 1, keys] + update
        state_ref[h] = state


def near_kernel(qk_ref, v_ref, in_ref, out_ref, far_ref, enter_ref, part_ref, qfar_ref):
    length = qk_ref.shape[0]
    heads, value_dim, key_dim = enter_ref.shape[1:]
    scale = key_dim ** (-0.5)
    low = lax.broadcasted_iota(jnp.int32, (BLOCK, BLOCK), 0)
    high = lax.broadcasted_iota(jnp.int32, (BLOCK, BLOCK), 1)
    causal = high <= low
    for n in range(length // BLOCK):
        rows = slice(n * BLOCK, (n + 1) * BLOCK)
        for h in range(heads):
            keys = slice(h * key_dim, (h + 1) * key_dim)
            lanes = slice((heads + h) * key_dim, (heads + h + 1) * key_dim)
            values = slice(h * value_dim, (h + 1) * value_dim)
            q = qk_ref[rows, keys].astype(F32) * scale
            qd = (q * in_ref[rows, keys]).astype(BF16)
            ki = (qk_ref[rows, lanes].astype(F32) * out_ref[rows, keys]).astype(BF16)
            qfar_ref[rows, keys] = (q * far_ref[rows, keys]).astype(BF16)
            scores = jnp.where(causal, across(qd, ki), 0.0).astype(BF16)
            part_ref[rows, values] = dot(scores, v_ref[rows, values]) + across(qd, enter_ref[n, h])


def local_states(qk, v, tail, end, heads):
    length, width = qk.shape[0], qk.shape[1] // 2
    shape = (heads, v.shape[1] // heads, width // heads)
    return vmem_kernel(
        state_kernel,
        (
            jax.ShapeDtypeStruct((length // BLOCK,) + shape, BF16),
            jax.ShapeDtypeStruct(shape, F32),
        ),
        1_000_000_000,
        qk,
        v,
        tail,
        end,
        in_specs=[pl.BlockSpec(memory_space=pltpu.VMEM)] * 4,
    )


def local_attention(qk, v, *terms):
    length, width = qk.shape[0], qk.shape[1] // 2
    return vmem_kernel(
        near_kernel,
        (
            jax.ShapeDtypeStruct((length, v.shape[1]), F32),
            jax.ShapeDtypeStruct((length, width), BF16),
        ),
        2_000_000_000,
        qk,
        v,
        *terms,
        in_specs=[pl.BlockSpec(memory_space=pltpu.VMEM)] * (2 + len(terms)),
    )


def finish_kernel(part_ref, qfar_ref, state_ref, gain_ref, mixed_ref):
    heads = state_ref.shape[0]
    key_dim = qfar_ref.shape[1] // heads
    value_dim = part_ref.shape[1] // heads
    for h in range(heads):
        keys = slice(h * key_dim, (h + 1) * key_dim)
        values = slice(h * value_dim, (h + 1) * value_dim)
        attended = part_ref[:, values] + across(qfar_ref[:, keys], state_ref[h])
        meansq = jnp.mean(attended * attended, axis=-1, keepdims=True)
        gain = gain_ref[h : h + 1].astype(F32)
        mixed_ref[:, values] = (attended * lax.rsqrt(meansq + EPSILON) * gain).astype(BF16)


def finish_attention(part, qfar, state, gain):
    length, wide = part.shape
    return vmem_kernel(
        finish_kernel,
        jax.ShapeDtypeStruct((length, wide), BF16),
        100_000_000,
        part,
        qfar,
        state,
        gain,
        in_specs=[pl.BlockSpec(memory_space=pltpu.VMEM)] * 4,
    )


def unpack(packed, value_dim):
    packed = packed.astype(F32)
    return packed[:, value_dim : value_dim + 1], packed[:, :value_dim]


def combine(earlier, later):
    return earlier[0] * later[0], later[0] * earlier[1] + later[1]


def pack(pair):
    decay, state = pair
    heads, _, key_dim = state.shape
    lines = jnp.broadcast_to(decay, (heads, 16, key_dim))
    return jnp.concatenate([state, lines], axis=1).astype(BF16)


def entering(decay, state):
    value_dim = state.shape[1]
    z, y = lax.axis_index("z"), lax.axis_index("y")
    own = pack((decay, state))
    empty = (jnp.ones_like(decay), jnp.zeros_like(state))

    def only(passed, pair):
        return tuple(jnp.where(passed, a, b) for a, b in zip(pair, empty))

    before = empty
    total = (decay, state)
    got = [unpack(hop(own, "y", step), value_dim) for step in (1, 2, 3)]
    for step in (1, 2, 3):
        pair = got[step - 1]
        before = combine(only(y >= step, pair), before)
    after = empty
    for step in (3, 2, 1):
        after = combine(after, only(y < step, got[step - 1]))
    total = combine(combine(before, total), after)
    line = pack(total)
    outer = empty
    for step in (1, 2, 3):
        pair = unpack(hop(line, "z", step), value_dim)
        outer = combine(only(z >= step, pair), outer)
    return combine(outer, before)[1].astype(BF16)


TILE = 1024


def targets(steps, part):
    x, c = lax.axis_index("x"), lax.axis_index("c")
    return [
        pl.multiple_of((lax.rem(x + step, RING) * PAIR + core) * part, HALO)
        for core in (1 - c, c)
        for step in steps
    ]


def stacked(refs, spots, part):
    lines = [[ref[pl.ds(at, part), :] for ref in refs] for at in spots]
    lines = [jnp.concatenate(line, axis=1) if len(line) > 1 else line[0] for line in lines]
    return jnp.concatenate(lines, axis=0)


def conv_kernel(groups, t_ref, b_ref, filter_ref, *outs):
    spots, part = [], outs[0].shape[0] // (PAIR * len(groups[0]))
    for steps in groups:
        spots += targets(steps, part)
    rows = stacked((t_ref, b_ref), spots, part)

    @pl.loop(0, filter_ref.shape[1] // TILE)
    def _(j):
        cols = pl.ds(pl.multiple_of(j * TILE, TILE), TILE)
        out = dot(rows, filter_ref[:, cols])
        at = 0
        for ref in outs:
            ref[:, cols] = out[at : at + ref.shape[0]]
            at += ref.shape[0]


def conv_call(groups, t, b, filt, part):
    return vmem_kernel(
        functools.partial(conv_kernel, groups),
        tuple(
            jax.ShapeDtypeStruct((PAIR * len(steps) * part, filt.shape[1]), F32)
            for steps in groups
        ),
        2_000_000_000,
        t,
        b,
        filt,
        in_specs=[pl.BlockSpec(memory_space=pltpu.VMEM)] * 3,
        out_specs=tuple(pl.BlockSpec(memory_space=pltpu.VMEM) for _ in groups),
    )


def term_kernel(steps, attn_ref, mixer_ref, acc_ref, own_ref, other_ref):
    count = own_ref.shape[0]
    part = count // len(steps)
    attn = stacked((attn_ref,), targets(steps, part), part)

    @pl.loop(0, own_ref.shape[1] // TILE)
    def _(j):
        cols = pl.ds(pl.multiple_of(j * TILE, TILE), TILE)
        out = acc_ref[:, cols] + dot(attn, mixer_ref[:, cols])
        other_ref[:, cols] = out[:count].astype(BF16)
        own_ref[:, cols] = out[count:]


def term_call(steps, attn, mixer, acc, part):
    width = mixer.shape[1]
    part = part * len(steps)
    whole = pl.BlockSpec(memory_space=pltpu.VMEM)
    return vmem_kernel(
        functools.partial(term_kernel, steps),
        (
            jax.ShapeDtypeStruct((part, width), F32),
            jax.ShapeDtypeStruct((part, width), BF16),
        ),
        2_000_000_000,
        attn,
        mixer,
        acc,
        in_specs=[whole] * 3,
        out_specs=(whole, whole),
    )


def plus(*terms):
    total = terms[0].astype(F32)
    for term in terms[1:]:
        total = total + term.astype(F32)
    return total


def body(
    hidden,
    entry_gain,
    probe,
    lookup,
    payload,
    postfilter,
    prefilter,
    source,
    forget_left,
    forget_right,
    forget_offset,
    forget_spike,
    head_gain,
    taps,
    mixer_result,
    filter_result,
):
    heads, value_dim = head_gain.shape
    key_dim = probe.shape[1] // heads
    channels = taps.shape[1]
    half = channels // 2
    keys, values = 2 * heads * key_dim, heads * value_dim

    def shard(attn, convs, cols):
        return jnp.concatenate(attn + [w[:, cols] for w in convs], axis=1)

    normed = norm_rows(hidden, entry_gain)
    part = normed.shape[0]
    rim = onward(normed[part - HALO :], SP, 1)
    convs = (postfilter, prefilter, source)
    tops = shard([probe, lookup], convs, slice(0, half))
    bottoms = shard([payload], lax.optimization_barrier(convs), slice(half, channels))
    first = around(tops, "z")
    second = around(bottoms, "y")
    x = gather_rows(jnp.concatenate([normed, rim], axis=0))

    line_qk, line_t = line_up("z", first, (keys, 3 * half))
    line_v, line_b = line_up("y", second, (values, 3 * half))
    w_qk = around(line_qk, "y")
    w_v = around(line_v, "z")
    w_t = around(line_t, "y")
    w_b = around(line_b, "z")

    in_decay, out_decay, tail, far_decay, end, total = decay_terms(x, forget_left, forget_right, forget_offset, forget_spike)
    total = total.reshape(heads, 1, key_dim)
    early, late = (0, 1, 2), (3, 4)
    acc_qk = project_call(x, None, w_qk[:3], early, 1, HALO, F32)
    acc_v = project_call(x, None, w_v[:3], early, 0, HALO, F32)
    qk = project_call(x, acc_qk, w_qk[3:], late, 1, HALO, BF16)
    v = project_call(x, acc_v, w_v[3:], late, 0, HALO, BF16)
    enter, state = local_states(qk, v, tail, end, heads)
    near, qfar = local_attention(qk, v, in_decay, out_decay, far_decay, enter)
    incoming = entering(total, state)
    mixed_attn = finish_attention(near, qfar, incoming, head_gain)

    acc_t = project_call(x, None, w_t[:3], early, 1, 0, F32)
    acc_b = project_call(x, None, w_b[:3], early, 0, 0, F32)
    mixed_t = gate_call(x, acc_t, w_t[3:], late, taps[:, :half], 1)
    mixed_b = gate_call(x, acc_b, w_b[3:], late, taps[:, half:], 0)

    groups = ((2,), (1, 3))
    shares = dict(zip(groups, conv_call(groups, mixed_t, mixed_b, filter_result, part)))

    def partial(*steps):
        share = shares.get(steps)
        if share is None:
            share = conv_call((steps,), mixed_t, mixed_b, filter_result, part)[0]
        own, other = term_call(steps, mixed_attn, mixer_result, share, part)
        return plus(own, swap(other))

    cut = part // 2
    far = partial(2).astype(BF16)
    far_up, far_down = hop(far[:cut], "x", 1), hop(far[cut:], "x", -1)
    near_terms = partial(1, 3)
    up, down = near_terms[:part], near_terms[part:]
    plain_up = hop(up[cut:].astype(BF16), "x", 1)
    plain_down = hop(down[:cut].astype(BF16), "x", -1)
    last_up = hop(plus(up[:cut], far_up).astype(BF16), "x", 1)
    last_down = hop(plus(down[cut:], far_down).astype(BF16), "x", -1)
    from_below = jnp.concatenate([last_up, plain_up], axis=0)
    from_above = jnp.concatenate([plain_down, last_down], axis=0)
    return plus(partial(0), from_below, from_above).astype(BF16)


def solution(mesh):
    split = Mesh(mesh.devices.reshape(RING, RING, RING, PAIR), ALL)
    in_specs = (
        P(ALL, None),
        P(),
        P(SP, TP),
        P(SP, TP),
        P(SP, TP),
        P(SP, TP),
        P(SP, TP),
        P(SP, TP),
        P(),
        P(None, TP),
        P(TP),
        P(TP, SP),
        P(TP, None),
        P(None, TP),
        P(TP, None),
        P(TP, None),
    )

    return jax.shard_map(
        body, mesh=split, in_specs=in_specs, out_specs=P(ALL, None), check_vma=False
    )
```

```python
import functools

import jax
import jax.numpy as jnp
from jax import lax
from jax.experimental import pallas as pl
from jax.experimental.pallas import tpu as pltpu
from jax.sharding import Mesh
from jax.sharding import PartitionSpec as P

BLOCK = 64
SP = ("z", "y")
TP = ("x", "c")
ALL = ("z", "y", "x", "c")
RING = 4
PAIR = 2
HALO = 16

EPSILON = 1e-06
SOFTNESS = 16.0

F32 = jnp.float32
BF16 = jnp.bfloat16


def dot(a, b):
    return jnp.dot(a, b, preferred_element_type=F32)


def hop(value, axis, steps):
    return lax.ppermute(value, axis, [(i, (i + steps) % RING) for i in range(RING)])


def swap(value):
    return lax.ppermute(value, "c", [(0, 1), (1, 0)])


def onward(value, axis, steps):
    count = RING * RING if axis == SP else RING
    return lax.ppermute(value, axis, [(i, i + steps) for i in range(count - steps)])


def around(value, axis, half=None):
    half = half or value.shape[0] // 2
    below, above = hop(value, axis, 1), hop(value, axis, -1)
    top = hop(below[:half], axis, 1)
    bottom = hop(above[half:], axis, -1)
    return value, below, above, top, bottom


def vmem_kernel(kernel, out_shape, flops, *args, **kwargs):
    return pl.pallas_call(
        kernel,
        out_shape=out_shape,
        compiler_params=pltpu.CompilerParams(vmem_limit_bytes=kwargs.pop("limit", 10) << 20),
        cost_estimate=pl.CostEstimate(
            flops=flops, bytes_accessed=8_000_000, transcendentals=0
        ),
        **kwargs,
    )(*args)


def line_kernel(axis, own, below, above, top, bottom, *outs):
    me = lax.axis_index(axis)
    rows = own.shape[0]
    half = rows // 2
    at = 0
    for out in outs:
        cols = slice(at, at + out.shape[1])
        at += out.shape[1]
        for ref, step, offset in (
            (own, 0, 0),
            (below, 3, 0),
            (above, 1, 0),
            (top, 2, 0),
            (bottom, 2, half),
        ):
            start = pl.multiple_of(lax.rem(me + step, RING) * rows + offset, half)
            out[pl.ds(start, ref.shape[0]), :] = ref[:, cols]


def line_up(axis, pieces, widths):
    rows = pieces[0].shape[0] * RING
    return vmem_kernel(
        functools.partial(line_kernel, axis),
        tuple(jax.ShapeDtypeStruct((rows, w), BF16) for w in widths),
        1_000_000_000,
        *pieces,
    )


def chips_kernel(own, below, above, top, bottom, out):
    x = lax.axis_index("x")
    rows = own.shape[0]
    half = top.shape[0]
    for ref, step, offset in (
        (own, 0, 0),
        (below, 3, 0),
        (above, 1, 0),
        (top, 2, 0),
        (bottom, 2, half),
    ):
        start = pl.multiple_of(lax.rem(x + step, RING) * rows + offset, HALO)
        out[pl.ds(start, ref.shape[0]), :] = ref[...]


def rows_kernel(mine, other, out):
    c = lax.axis_index("c")
    block = mine.shape[0] // RING
    part = block - HALO
    for ref, core in ((mine, c), (other, 1 - c)):
        for chip in range(RING):
            start = pl.multiple_of(HALO + (chip * PAIR + core) * part, HALO)
            out[pl.ds(start, part), :] = ref[chip * block : chip * block + part]

        @pl.when(core == 1)
        def _(ref=ref):
            out[:HALO] = ref[RING * block - HALO :]


def gather_rows(shard):
    block, width = shard.shape
    part = block - HALO
    pieces = around(shard, "x", part // 2)
    mine = vmem_kernel(
        chips_kernel,
        jax.ShapeDtypeStruct((RING * block, width), BF16),
        1_000_000_000,
        *pieces,
        limit=16,
    )
    return vmem_kernel(
        rows_kernel,
        jax.ShapeDtypeStruct((HALO + RING * PAIR * part, width), BF16),
        2_000_000_000,
        mine,
        swap(mine),
        limit=16,
    )


def project(x_ref, lead, along, pieces, which, block):
    me = lax.axis_index("z" if along == 0 else "y")
    total = None
    for ref, index in zip(pieces, which):
        step, first = ((0, 0), (3, 0), (1, 0), (2, 0), (2, 2))[index]
        where = lax.rem(me + step, RING)
        count = ref.shape[0] // block
        if along == 0:
            start = pl.multiple_of((where * RING + first) * block, block)
            term = dot(x_ref[lead:, pl.ds(start, count * block)], ref[...])
            total = term if total is None else total + term
        else:
            for i in range(count):
                start = pl.multiple_of(((first + i) * RING + where) * block, block)
                term = dot(
                    x_ref[lead:, pl.ds(start, block)], ref[i * block : (i + 1) * block, :]
                )
                total = term if total is None else total + term
    return total


def project_kernel(lead, along, which, block, x_ref, *refs):
    *pieces, out = refs
    out[...] = project(x_ref, lead, along, pieces, which, block).astype(out.dtype)


def project_more_kernel(lead, along, which, block, x_ref, acc_ref, *refs):
    *pieces, out = refs
    total = acc_ref[...] + project(x_ref, lead, along, pieces, which, block)
    out[...] = total.astype(out.dtype)


def project_call(x, acc, pieces, which, along, lead, dtype, tile=256):
    block = x.shape[1] // (RING * RING)
    rows = x.shape[0] - lead
    width = pieces[0].shape[1]
    more = () if acc is None else (acc,)
    kernel = project_kernel if acc is None else project_more_kernel
    return vmem_kernel(
        functools.partial(kernel, lead, along, which, block),
        jax.ShapeDtypeStruct((rows, width), dtype),
        3_000_000_000,
        x,
        *more,
        *pieces,
        grid=(width // tile,),
        in_specs=[pl.BlockSpec(memory_space=pltpu.VMEM)]
        + [pl.BlockSpec((rows, tile), lambda i: (0, i)) for _ in more]
        + [pl.BlockSpec((p.shape[0], tile), lambda i: (0, i)) for p in pieces],
        out_specs=pl.BlockSpec((rows, tile), lambda i: (0, i)),
    )


def gate_kernel(along, which, block, x_ref, acc_ref, *refs):
    *pieces, taps_ref, out = refs
    sums = (acc_ref[...] + project(x_ref, 0, along, pieces, which, block)).astype(BF16)
    width = sums.shape[1] // 3
    length = sums.shape[0] - HALO
    gated = (sums[:, width : 2 * width].astype(F32) * sums[:, 2 * width :].astype(F32)).astype(BF16)
    gated = gated.astype(F32)
    taps = taps_ref.shape[0]
    conv = jnp.zeros((length, width), F32)
    for i in range(taps):
        lead = HALO + 1 - taps + i
        conv = conv + taps_ref[i : i + 1, :].astype(F32) * gated[lead : lead + length]
    out[...] = (conv * sums[HALO:, :width].astype(F32)).astype(BF16)


def gate_call(x, acc, pieces, which, taps, along):
    block = x.shape[1] // (RING * RING)
    return vmem_kernel(
        functools.partial(gate_kernel, along, which, block),
        jax.ShapeDtypeStruct((x.shape[0] - HALO, taps.shape[1]), BF16),
        2_000_000_000,
        x,
        acc,
        *pieces,
        taps,
        in_specs=[pl.BlockSpec(memory_space=pltpu.VMEM)] * (3 + len(pieces)),
        out_specs=pl.BlockSpec(memory_space=pltpu.VMEM),
    )


def norm_kernel(rows_ref, gain_ref, out_ref):
    rows = rows_ref[...].astype(F32)
    meansq = jnp.mean(rows * rows, axis=-1, keepdims=True)
    normed = rows * lax.rsqrt(meansq + EPSILON) * gain_ref[...].astype(F32)[None]
    out_ref[...] = normed.astype(BF16)


def norm_rows(rows, gain):
    return vmem_kernel(norm_kernel, jax.ShapeDtypeStruct(rows.shape, BF16), 1_000_000, rows, gain)


def decay_kernel(
    x_ref, left_ref, right_ref, offset_ref, spike_ref, in_ref, out_ref, tail_ref, far_ref, end_ref, total_ref
):
    length, width = in_ref.shape
    heads = spike_ref.shape[0]
    low_rank = across(x_ref[HALO:, :], left_ref[...]).astype(BF16)
    gate = dot(low_rank, right_ref[...]) + offset_ref[...]
    soft = jnp.minimum(gate, 0.0) - jnp.log1p(jnp.exp(-jnp.abs(gate)))
    head = lax.broadcasted_iota(jnp.int32, (heads, width), 0)
    feature = lax.broadcasted_iota(jnp.int32, (heads, width), 1)
    owner = jnp.where(feature // (width // heads) == head, 1.0, 0.0).astype(F32)
    spikes = lax.dot_general(
        spike_ref[...],
        owner,
        (((0,), (0,)), ((), ())),
        preferred_element_type=F32,
        precision=lax.Precision.HIGHEST,
    )
    rate = soft / SOFTNESS + spikes
    low = lax.broadcasted_iota(jnp.int32, (BLOCK, BLOCK), 0)
    high = lax.broadcasted_iota(jnp.int32, (BLOCK, BLOCK), 1)
    tri = jnp.where(high <= low, 1.0, 0.0).astype(F32)
    prefix = jnp.zeros((1, width), F32)
    tail_ref[...] = rate

    def step(n, prefix):
        rows = pl.ds(pl.multiple_of(n * BLOCK, BLOCK), BLOCK)
        within = jnp.dot(
            tri, tail_ref[rows, :], preferred_element_type=F32, precision=lax.Precision.HIGHEST
        )
        end = within[BLOCK - 1 :]
        grow = jnp.exp(within)
        in_ref[rows, :] = grow
        out_ref[rows, :] = jnp.exp(-within)
        tail_ref[rows, :] = jnp.exp(end - within)
        far_ref[rows, :] = grow * jnp.exp(prefix)
        end_ref[pl.ds(n, 1), :] = jnp.exp(end)
        return prefix + end

    total_ref[...] = jnp.exp(lax.fori_loop(0, length // BLOCK, step, prefix))


def decay_terms(x, left, right, offset, spike):
    length, width = x.shape[0] - HALO, right.shape[1]
    full = jax.ShapeDtypeStruct((length, width), F32)
    return vmem_kernel(
        decay_kernel,
        (
            full,
            full,
            full,
            full,
            jax.ShapeDtypeStruct((length // BLOCK, width), F32),
            jax.ShapeDtypeStruct((1, width), F32),
        ),
        4_000_000_000,
        x,
        jnp.transpose(left),
        right,
        offset[None],
        spike,
        in_specs=[pl.BlockSpec(memory_space=pltpu.VMEM)] * 5,
    )


def across(a, b):
    return lax.dot_general(a, b, (((1,), (1,)), ((), ())), preferred_element_type=F32)


def state_kernel(qk_ref, v_ref, tail_ref, end_ref, enter_ref, state_ref):
    heads, value_dim, key_dim = state_ref.shape
    for h in range(heads):
        keys = slice(h * key_dim, (h + 1) * key_dim)
        lanes = slice((heads + h) * key_dim, (heads + h + 1) * key_dim)
        values = slice(h * value_dim, (h + 1) * value_dim)
        state = jnp.zeros((value_dim, key_dim), F32)
        for n in range(v_ref.shape[0] // BLOCK):
            rows = slice(n * BLOCK, (n + 1) * BLOCK)
            enter_ref[n, h] = state.astype(BF16)
            kt = (qk_ref[rows, lanes].astype(F32) * tail_ref[rows, keys]).astype(BF16)
            update = lax.dot_general(
                v_ref[rows, values], kt, (((0,), (0,)), ((), ())), preferred_element_type=F32
            )
            state = state * end_ref[n : n + 1, keys] + update
        state_ref[h] = state


def near_kernel(qk_ref, v_ref, in_ref, out_ref, far_ref, enter_ref, part_ref, qfar_ref):
    length = qk_ref.shape[0]
    heads, value_dim, key_dim = enter_ref.shape[1:]
    scale = key_dim ** (-0.5)
    low = lax.broadcasted_iota(jnp.int32, (BLOCK, BLOCK), 0)
    high = lax.broadcasted_iota(jnp.int32, (BLOCK, BLOCK), 1)
    causal = high <= low
    for n in range(length // BLOCK):
        rows = slice(n * BLOCK, (n + 1) * BLOCK)
        for h in range(heads):
            keys = slice(h * key_dim, (h + 1) * key_dim)
            lanes = slice((heads + h) * key_dim, (heads + h + 1) * key_dim)
            values = slice(h * value_dim, (h + 1) * value_dim)
            q = qk_ref[rows, keys].astype(F32) * scale
            qd = (q * in_ref[rows, keys]).astype(BF16)
            ki = (qk_ref[rows, lanes].astype(F32) * out_ref[rows, keys]).astype(BF16)
            qfar_ref[rows, keys] = (q * far_ref[rows, keys]).astype(BF16)
            scores = jnp.where(causal, across(qd, ki), 0.0).astype(BF16)
            part_ref[rows, values] = dot(scores, v_ref[rows, values]) + across(qd, enter_ref[n, h])


def local_states(qk, v, tail, end, heads):
    length, width = qk.shape[0], qk.shape[1] // 2
    shape = (heads, v.shape[1] // heads, width // heads)
    return vmem_kernel(
        state_kernel,
        (
            jax.ShapeDtypeStruct((length // BLOCK,) + shape, BF16),
            jax.ShapeDtypeStruct(shape, F32),
        ),
        1_000_000_000,
        qk,
        v,
        tail,
        end,
        in_specs=[pl.BlockSpec(memory_space=pltpu.VMEM)] * 4,
    )


def local_attention(qk, v, *terms):
    length, width = qk.shape[0], qk.shape[1] // 2
    return vmem_kernel(
        near_kernel,
        (
            jax.ShapeDtypeStruct((length, v.shape[1]), F32),
            jax.ShapeDtypeStruct((length, width), BF16),
        ),
        2_000_000_000,
        qk,
        v,
        *terms,
        in_specs=[pl.BlockSpec(memory_space=pltpu.VMEM)] * (2 + len(terms)),
    )


def finish_kernel(part_ref, qfar_ref, state_ref, gain_ref, mixed_ref):
    heads = state_ref.shape[0]
    key_dim = qfar_ref.shape[1] // heads
    value_dim = part_ref.shape[1] // heads
    for h in range(heads):
        keys = slice(h * key_dim, (h + 1) * key_dim)
        values = slice(h * value_dim, (h + 1) * value_dim)
        attended = part_ref[:, values] + across(qfar_ref[:, keys], state_ref[h])
        meansq = jnp.mean(attended * attended, axis=-1, keepdims=True)
        gain = gain_ref[h : h + 1].astype(F32)
        mixed_ref[:, values] = (attended * lax.rsqrt(meansq + EPSILON) * gain).astype(BF16)


def finish_attention(part, qfar, state, gain):
    length, wide = part.shape
    return vmem_kernel(
        finish_kernel,
        jax.ShapeDtypeStruct((length, wide), BF16),
        100_000_000,
        part,
        qfar,
        state,
        gain,
        in_specs=[pl.BlockSpec(memory_space=pltpu.VMEM)] * 4,
    )


def unpack(packed, value_dim):
    packed = packed.astype(F32)
    return packed[:, value_dim : value_dim + 1], packed[:, :value_dim]


def combine(earlier, later):
    return earlier[0] * later[0], later[0] * earlier[1] + later[1]


def pack(pair):
    decay, state = pair
    heads, _, key_dim = state.shape
    lines = jnp.broadcast_to(decay, (heads, 16, key_dim))
    return jnp.concatenate([state, lines], axis=1).astype(BF16)


def entering(decay, state):
    value_dim = state.shape[1]
    z, y = lax.axis_index("z"), lax.axis_index("y")
    own = pack((decay, state))
    empty = (jnp.ones_like(decay), jnp.zeros_like(state))

    def only(passed, pair):
        return tuple(jnp.where(passed, a, b) for a, b in zip(pair, empty))

    before = empty
    total = (decay, state)
    got = [unpack(hop(own, "y", step), value_dim) for step in (1, 2, 3)]
    for step in (1, 2, 3):
        pair = got[step - 1]
        before = combine(only(y >= step, pair), before)
    after = empty
    for step in (3, 2, 1):
        after = combine(after, only(y < step, got[step - 1]))
    total = combine(combine(before, total), after)
    line = pack(total)
    outer = empty
    for step in (1, 2, 3):
        pair = unpack(hop(line, "z", step), value_dim)
        outer = combine(only(z >= step, pair), outer)
    return combine(outer, before)[1].astype(BF16)


TILE = 1024


def targets(steps, part):
    x, c = lax.axis_index("x"), lax.axis_index("c")
    return [
        pl.multiple_of((lax.rem(x + step, RING) * PAIR + core) * part, HALO)
        for core in (1 - c, c)
        for step in steps
    ]


def stacked(refs, spots, part):
    lines = [[ref[pl.ds(at, part), :] for ref in refs] for at in spots]
    lines = [jnp.concatenate(line, axis=1) if len(line) > 1 else line[0] for line in lines]
    return jnp.concatenate(lines, axis=0)


def conv_kernel(groups, t_ref, b_ref, filter_ref, mixer_ref, *outs):
    spots, part = [], outs[0].shape[0] // (PAIR * len(groups[0]))
    for steps in groups:
        spots += targets(steps, part)
    rows = stacked((t_ref, b_ref), spots, part)

    @pl.loop(0, filter_ref.shape[1] // TILE)
    def _(j):
        cols = pl.ds(pl.multiple_of(j * TILE, TILE), TILE)
        out = dot(rows, filter_ref[:, cols])
        at = 0
        for ref in outs:
            ref[:, cols] = out[at : at + ref.shape[0]]
            at += ref.shape[0]


def conv_call(groups, t, b, filt, mixer, part):
    return vmem_kernel(
        functools.partial(conv_kernel, groups),
        tuple(
            jax.ShapeDtypeStruct((PAIR * len(steps) * part, filt.shape[1]), F32)
            for steps in groups
        ),
        2_000_000_000,
        t,
        b,
        filt,
        mixer,
        in_specs=[pl.BlockSpec(memory_space=pltpu.VMEM)] * 4,
        out_specs=tuple(pl.BlockSpec(memory_space=pltpu.VMEM) for _ in groups),
    )


def term_kernel(steps, attn_ref, mixer_ref, acc_ref, own_ref, other_ref):
    count = own_ref.shape[0]
    part = count // len(steps)
    attn = stacked((attn_ref,), targets(steps, part), part)

    @pl.loop(0, own_ref.shape[1] // TILE)
    def _(j):
        cols = pl.ds(pl.multiple_of(j * TILE, TILE), TILE)
        out = acc_ref[:, cols] + dot(attn, mixer_ref[:, cols])
        other_ref[:, cols] = out[:count].astype(BF16)
        own_ref[:, cols] = out[count:]


def term_call(steps, attn, mixer, acc, part):
    width = mixer.shape[1]
    part = part * len(steps)
    whole = pl.BlockSpec(memory_space=pltpu.VMEM)
    return vmem_kernel(
        functools.partial(term_kernel, steps),
        (
            jax.ShapeDtypeStruct((part, width), F32),
            jax.ShapeDtypeStruct((part, width), BF16),
        ),
        2_000_000_000,
        attn,
        mixer,
        acc,
        in_specs=[whole] * 3,
        out_specs=(whole, whole),
    )


def plus(*terms):
    total = terms[0].astype(F32)
    for term in terms[1:]:
        total = total + term.astype(F32)
    return total


def body(
    hidden,
    entry_gain,
    probe,
    lookup,
    payload,
    postfilter,
    prefilter,
    source,
    forget_left,
    forget_right,
    forget_offset,
    forget_spike,
    head_gain,
    taps,
    mixer_result,
    filter_result,
):
    heads, value_dim = head_gain.shape
    key_dim = probe.shape[1] // heads
    channels = taps.shape[1]
    half = channels // 2
    keys, values = 2 * heads * key_dim, heads * value_dim

    def shard(attn, convs, cols):
        return jnp.concatenate(attn + [w[:, cols] for w in convs], axis=1)

    normed = norm_rows(hidden, entry_gain)
    part = normed.shape[0]
    rim = onward(normed[part - HALO :], SP, 1)
    convs = (postfilter, prefilter, source)
    tops = shard([probe, lookup], convs, slice(0, half))
    bottoms = shard([payload], lax.optimization_barrier(convs), slice(half, channels))
    first = around(tops, "z")
    second = around(bottoms, "y")
    x = gather_rows(jnp.concatenate([normed, rim], axis=0))

    line_qk, line_t = line_up("z", first, (keys, 3 * half))
    line_v, line_b = line_up("y", second, (values, 3 * half))
    w_qk = around(line_qk, "y")
    w_v = around(line_v, "z")
    w_t = around(line_t, "y")
    w_b = around(line_b, "z")

    in_decay, out_decay, tail, far_decay, end, total = decay_terms(x, forget_left, forget_right, forget_offset, forget_spike)
    total = total.reshape(heads, 1, key_dim)
    early, late = (0, 1, 2), (3, 4)
    acc_qk = project_call(x, None, w_qk[:3], early, 1, HALO, F32)
    acc_v = project_call(x, None, w_v[:3], early, 0, HALO, F32)
    qk = project_call(x, acc_qk, w_qk[3:], late, 1, HALO, BF16)
    v = project_call(x, acc_v, w_v[3:], late, 0, HALO, BF16)
    enter, state = local_states(qk, v, tail, end, heads)
    near, qfar = local_attention(qk, v, in_decay, out_decay, far_decay, enter)
    incoming = entering(total, state)
    mixed_attn = finish_attention(near, qfar, incoming, head_gain)

    acc_t = project_call(x, None, w_t[:3], early, 1, 0, F32)
    acc_b = project_call(x, None, w_b[:3], early, 0, 0, F32)
    mixed_t = gate_call(x, acc_t, w_t[3:], late, taps[:, :half], 1)
    mixed_b = gate_call(x, acc_b, w_b[3:], late, taps[:, half:], 0)

    groups = ((2,), (1, 3))
    shares = dict(zip(groups, conv_call(groups, mixed_t, mixed_b, filter_result, mixer_result, part)))

    def partial(*steps):
        share = shares.get(steps)
        if share is None:
            share = conv_call((steps,), mixed_t, mixed_b, filter_result, mixer_result, part)[0]
        own, other = term_call(steps, mixed_attn, mixer_result, share, part)
        return plus(own, swap(other))

    cut = part // 2
    far = partial(2).astype(BF16)
    far_up, far_down = hop(far[:cut], "x", 1), hop(far[cut:], "x", -1)
    near_terms = partial(1, 3)
    up, down = near_terms[:part], near_terms[part:]
    plain_up = hop(up[cut:].astype(BF16), "x", 1)
    plain_down = hop(down[:cut].astype(BF16), "x", -1)
    last_up = hop(plus(up[:cut], far_up).astype(BF16), "x", 1)
    last_down = hop(plus(down[cut:], far_down).astype(BF16), "x", -1)
    from_below = jnp.concatenate([last_up, plain_up], axis=0)
    from_above = jnp.concatenate([plain_down, last_down], axis=0)
    return plus(partial(0), from_below, from_above).astype(BF16)


def solution(mesh):
    split = Mesh(mesh.devices.reshape(RING, RING, RING, PAIR), ALL)
    in_specs = (
        P(ALL, None),
        P(),
        P(SP, TP),
        P(SP, TP),
        P(SP, TP),
        P(SP, TP),
        P(SP, TP),
        P(SP, TP),
        P(),
        P(None, TP),
        P(TP),
        P(TP, SP),
        P(TP, None),
        P(None, TP),
        P(TP, None),
        P(TP, None),
    )

    return jax.shard_map(
        body, mesh=split, in_specs=in_specs, out_specs=P(ALL, None), check_vma=False
    )
```
